32 devices in a mesh: fs: 8 (over z, x), tp: 4 (over y, core).
Axes of the slice: x: 2, y: 2, z: 4, core: 2. Of those that a mesh axis runs over, the one named last changes fastest.
Arguments:
- later_rows: bfloat16 [3584, 2048], P(('fs', 'tp')), may hold values from -6 to 6
- earlier_rows: bfloat16 [3584, 2048], P(('fs', 'tp')), may hold values from -6 to 6
- cotangent: bfloat16 [3584, 2048], P(('fs', 'tp')), may hold values from -1 to 1
- gate_weight: bfloat16 [2048, 5632], P('fs', 'tp'), may hold values from -0.125 to 0.125
- up_weight: bfloat16 [2048, 5632], P('fs', 'tp'), may hold values from -0.125 to 0.125
- down_weight: bfloat16 [2048, 5632], P('fs', 'tp'), may hold values from -0.078125 to 0.078125
- gate_grad_sum: float32 [2048, 5632], P('fs', 'tp'), may hold values from -12 to 12
- up_grad_sum: float32 [2048, 5632], P('fs', 'tp'), may hold values from -12 to 12
- down_grad_sum: float32 [2048, 5632], P('fs', 'tp'), may hold values from -12 to 12
Outputs:
- later_out: bfloat16 [3584, 2048], P(('fs', 'tp'))
- input_grad: bfloat16 [3584, 2048], P(('fs', 'tp'))
- gate_grad_new: float32 [2048, 5632], P('fs', 'tp')
- up_grad_new: float32 [2048, 5632], P('fs', 'tp')
- down_grad_new: float32 [2048, 5632], P('fs', 'tp')
The draws below stay inside these ranges and needn't reach their ends.
All inputs are finite; a program needn't handle non-finite values.
Results may differ from the reference program's by a relative error of at most 0.014.
Values may be sent and summed in bfloat16 or wider, within the bound.
A program may use at most 128 MiB of HBM per device.

```python
import jax
import jax.numpy as jnp
from jax import lax

D = 2048
FF = 5632
TOKENS = 3584
N_TP = 4


def strengthened(values, stream_key, source, target, parts, factor):
    def block_of(position):
        return (jnp.arange(values.shape[position]) // (values.shape[position] // parts)).reshape((-1,) + (1,) * (values.ndim - 1 - position))

    first = jax.random.permutation(stream_key, parts)[block_of(target)]
    other_side = (block_of(target) + parts // 2) % parts
    return jnp.where((block_of(source) == first) | (block_of(source) == other_side), factor * values, values)


def block_scale(rng, shape, split, smallest, high):
    gain = 1.0
    for axis_at, shards_of in split:
        heights = jax.random.uniform(jax.random.fold_in(jax.random.fold_in(rng, 6), axis_at), (shards_of,), jnp.float32, smallest / len(split), high / len(split))
        gain = gain * jnp.repeat(jnp.exp(heights), shape[axis_at] // shards_of).reshape((-1,) + (1,) * (len(shape) - 1 - axis_at))
    return gain


def scatter_about(stream_key, shape, spread, limit, cuts=(), kind=jnp.bfloat16):
    drawn = jax.random.normal(stream_key, shape, jnp.float32) * spread
    if len(cuts) > 0:
        drawn = block_scale(stream_key, shape, cuts, -0.22, 0.18) * drawn
    return jnp.clip(drawn, min=-limit, max=limit).astype(kind)


def noise_with(rng, dims, spread, most, shards, heavy, held_as=jnp.bfloat16):
    drawn = spread * jax.random.normal(rng, dims, jnp.float32)
    if shards:
        drawn = drawn * block_scale(rng, dims, shards, -0.22, 0.18)
    return jnp.clip(strengthened(drawn, jax.random.fold_in(rng, 3), *heavy), -most, most).astype(held_as)


def setup_inputs(seed: int = 0) -> dict:
    streams_of = jax.random.split(jax.random.key(seed), 10)
    return {
        "later_rows": scatter_about(streams_of[0], (TOKENS, D), 1.0, 6.0, ((0, 32),)),
        "earlier_rows": scatter_about(streams_of[1], (TOKENS, D), 1.0, 6.0, ((0, 32),)),
        "cotangent": noise_with(streams_of[2], (TOKENS, D), 0.1, 1.0, ((0, 32),), (0, 1, 32, 2.75)),
        "gate_weight": scatter_about(streams_of[3], (D, FF), D ** -0.5, 0.125, ((0, 8), (1, 4))),
        "up_weight": scatter_about(streams_of[4], (D, FF), D ** -0.5, 0.125, ((0, 8), (1, 4))),
        "down_weight": scatter_about(streams_of[5], (D, FF), FF ** -0.5, 0.078125, ((0, 8), (1, 4))),
        "gate_grad_sum": scatter_about(streams_of[6], (D, FF), 2.0, 12.0, ((0, 8), (1, 4)), jnp.float32),
        "up_grad_sum": scatter_about(streams_of[7], (D, FF), 2.0, 12.0, ((0, 8), (1, 4)), jnp.float32),
        "down_grad_sum": scatter_about(streams_of[8], (D, FF), 2.0, 12.0, ((0, 8), (1, 4)), jnp.float32),
    }


def silu_parts(gate):
    sigma = jax.nn.sigmoid(gate)
    return gate * sigma, sigma * (1.0 + gate * (1.0 - sigma))


def by_columns(left, right):
    return lax.dot_general(left, right, (((1,), (1,)), ((), ())), preferred_element_type=jnp.float32)


def by_rows(left, right):
    return lax.dot_general(left, right, (((0,), (0,)), ((), ())), preferred_element_type=jnp.float32)


def reference(later_rows, earlier_rows, cotangent, gate_weight, up_weight, down_weight, gate_grad_sum, up_grad_sum, down_grad_sum):
    width = FF // N_TP
    later_gate = jnp.dot(later_rows, gate_weight, preferred_element_type=jnp.float32)
    later_up = jnp.dot(later_rows, up_weight, preferred_element_type=jnp.float32)
    later_hidden = (jax.nn.silu(later_gate) * later_up).astype(jnp.bfloat16)
    total = jnp.zeros((later_rows.shape[0], D), jnp.float32)
    for block in range(N_TP):
        lower = block * width
        part = by_columns(later_hidden[:, lower:lower + width], down_weight[:, lower:lower + width]).astype(jnp.bfloat16)
        total = total + lax.optimization_barrier(part).astype(jnp.float32)
    later_out = total.astype(jnp.bfloat16)

    gate_e = jnp.dot(earlier_rows, gate_weight, preferred_element_type=jnp.float32)
    up_e = jnp.dot(earlier_rows, up_weight, preferred_element_type=jnp.float32)
    activation, slope = silu_parts(gate_e)
    hidden_e = (activation * up_e).astype(jnp.bfloat16)
    back_hidden = jnp.dot(cotangent, down_weight, preferred_element_type=jnp.float32)
    gate_back = (back_hidden * up_e * slope).astype(jnp.bfloat16)
    up_back = (back_hidden * activation).astype(jnp.bfloat16)
    total = jnp.zeros((earlier_rows.shape[0], D), jnp.float32)
    for block in range(N_TP):
        lower = block * width
        part = by_columns(gate_back[:, lower:lower + width], gate_weight[:, lower:lower + width])
        part = part + by_columns(up_back[:, lower:lower + width], up_weight[:, lower:lower + width])
        total = total + lax.optimization_barrier(part.astype(jnp.bfloat16)).astype(jnp.float32)
    input_grad = total.astype(jnp.bfloat16)
    gate_grad_new = gate_grad_sum + by_rows(earlier_rows, gate_back)
    up_grad_new = up_grad_sum + by_rows(earlier_rows, up_back)
    down_grad_new = down_grad_sum + by_rows(cotangent, hidden_e)
    return later_out, input_grad, gate_grad_new, up_grad_new, down_grad_new
```

```python
import functools

import jax
import jax.numpy as jnp
from jax import lax
from jax.experimental import pallas as pl
from jax.experimental.pallas import tpu as pltpu
from jax.sharding import Mesh, PartitionSpec as P


def silu_parts(gate):
    sigma = jax.nn.sigmoid(gate)
    return (gate * sigma, sigma * (1.0 + gate * (1.0 - sigma)))


def by_columns(left, right):
    return lax.dot_general(
        left, right, (((1,), (1,)), ((), ())), preferred_element_type=jnp.float32
    )


def by_rows(left, right):
    return lax.dot_general(
        left, right, (((0,), (0,)), ((), ())), preferred_element_type=jnp.float32
    )


def dot(left, right):
    return jnp.dot(left, right, preferred_element_type=jnp.float32)


def pick(index, choices):
    value = choices[-1]
    for at in range(len(choices) - 2, -1, -1):
        value = jnp.where(index == at, choices[at], value)
    return value


def shift(value, axis, size, by):
    return lax.ppermute(value, axis, [(i, (i + by) % size) for i in range(size)])


def spread_columns(weight, nx):
    x = lax.axis_index("x")
    rows, columns = weight.shape[0], weight.shape[1] // nx
    parts = [weight[:, c * columns : (c + 1) * columns] for c in range(nx)]
    whole = [pick(x, parts)]
    for by in range(1, nx):
        whole.append(shift(pick((x + by) % nx, parts), "x", nx, by))
    return jnp.concatenate([pick((x - c) % nx, whole) for c in range(nx)], axis=0)


def join_columns(total, nx):
    x = lax.axis_index("x")
    rows = total.shape[0] // nx
    parts = [total[c * rows : (c + 1) * rows] for c in range(nx)]
    whole = [pick(x, parts)]
    for by in range(1, nx):
        sent = pick((x + by) % nx, parts).astype(jnp.bfloat16)
        whole.append(shift(sent, "x", nx, by).astype(jnp.float32))
    return jnp.concatenate([pick((x - c) % nx, whole) for c in range(nx)], axis=1)


def after(value, *earlier):
    return lax.optimization_barrier((value,) + earlier)[0]


def gather_line(block, nz, middle=lambda: ((), ())):
    z = lax.axis_index("z")
    ahead_step, ahead_use = middle()
    up = down = block
    ups, downs = [block], [block]
    for step in range(1, nz):
        if step == nz - 1 and ahead_step:
            up, down = after(up, *ahead_step), after(down, *ahead_step)
        up = lax.ppermute(up, "z", [(i, i + 1) for i in range(step - 1, nz - 1)])
        down = lax.ppermute(down, "z", [(i, i - 1) for i in range(1, nz - step + 1)])
        ups.append(up)
        downs.append(down)
    rows = block.shape[0]
    whole = jnp.zeros((nz * rows, block.shape[1]), block.dtype)
    whole = lax.dynamic_update_slice_in_dim(whole, block, z * rows, 0)
    for back in range(1, nz):
        arrived = jnp.where(z >= back, ups[back], downs[nz - back])
        if ahead_use:
            arrived = after(arrived, *ahead_use)
        whole = lax.dynamic_update_slice_in_dim(whole, arrived, ((z - back) % nz) * rows, 0)
    return whole, (ups[max(nz - 2, 0)], downs[max(nz - 2, 0)])


def scatter_line(parts, nz):
    z = lax.axis_index("z")
    rows = parts.shape[0] // nz

    def block(index):
        return lax.dynamic_slice_in_dim(parts, (index % nz) * rows, rows, 0)

    up = down = None
    first = ()
    for step in range(1, nz):
        up_sum, down_sum = block(z - step), block(z + step)
        if step > 1:
            up_sum = up_sum + up.astype(jnp.float32)
            down_sum = down_sum + down.astype(jnp.float32)
        up = lax.ppermute(
            up_sum.astype(jnp.bfloat16), "z", [(i, i + 1) for i in range(min(step, nz - 1))]
        )
        down = lax.ppermute(
            down_sum.astype(jnp.bfloat16), "z", [(i, i - 1) for i in range(max(nz - step, 1), nz)]
        )
        first = first or (up, down)
    total = block(z)
    if nz > 1:
        total = total + up.astype(jnp.float32) + down.astype(jnp.float32)
    return total, first


MESH = pl.DeviceIdType.MESH
TOKENS_IN = 3
WEIGHTS = 3


def fused_kernel(
    nz,
    width,
    ahead,
    row_tile,
    later_ref,
    earlier_ref,
    cotangent_ref,
    gate_ref,
    up_ref,
    down_ref,
    later_out_ref,
    input_grad_ref,
    gate_sum_ref,
    up_sum_ref,
    down_sum_ref,
    full,
    tokens,
    other_tokens,
    turned,
    acts,
    sums,
    later_acc,
    input_acc,
    parts_in,
    final,
    dots,
    own_sem,
    swap_send,
    swap_recv,
    line_recv,
    pair_recv,
    up_send,
    down_send,
    pair_send,
    token_own,
    token_send,
    token_recv,
    other_send,
    other_recv,
    act_send,
    act_recv,
    sum_send,
    sum_recv,
    final_send,
    final_recv,
    part_send,
    part_recv,
    out_sem,
):
    z, x, y, c = (lax.axis_index(name) for name in ("z", "x", "y", "c"))
    rows = later_ref.shape[0]
    depth, ff = gate_ref.shape
    model = later_ref.shape[1]
    half = tokens.shape[1]
    chunks = -(-ff // width)
    tail = ff - (chunks - 1) * width

    above, below = (z + 1, x, y, c), (z - 1, x, y, c)
    pair = (z, x, y, 1 - c)
    flip_x, flip_y, flip_both = (z, 1 - x, y, c), (z, x, 1 - y, c), (z, 1 - x, 1 - y, c)
    partner = (z, 1 - x, y, 1 - c)
    chip = 2 * x + y
    chip_x, chip_y, chip_both = 2 * (1 - x) + y, 2 * x + 1 - y, 2 * (1 - x) + 1 - y
    native = c == x
    has_above, has_below = z < nz - 1, z > 0

    weights = (gate_ref, up_ref, down_ref)
    token_refs = (earlier_ref, cotangent_ref, later_ref)

    def remote(src, dst, send, recv, device):
        return pltpu.make_async_remote_copy(
            src_ref=src, dst_ref=dst, send_sem=send, recv_sem=recv, device_id=device, device_id_type=MESH
        )

    def each(k, body):
        if tail == width:
            body(k, width)
            return

        @pl.when(k < chunks - 1)
        def _():
            body(k, width)

        @pl.when(k == chunks - 1)
        def _():
            body(k, tail)

    def columns(k, size):
        return pl.ds(pl.multiple_of(k * width, 128), size)

    def block_rows(block, parity):
        return pl.ds(pl.multiple_of((block * 2 + parity) * depth, depth), depth)

    def slot(index):
        return pl.ds(pl.multiple_of(index * rows, rows), rows)

    barrier = pltpu.get_barrier_semaphore()
    for device in (pair, flip_x, flip_y, flip_both, partner):
        pl.semaphore_signal(barrier, inc=1, device_id=device, device_id_type=MESH)

    @pl.when(has_above)
    def _():
        pl.semaphore_signal(barrier, inc=1, device_id=above, device_id_type=MESH)

    @pl.when(has_below)
    def _():
        pl.semaphore_signal(barrier, inc=1, device_id=below, device_id_type=MESH)

    pl.semaphore_wait(barrier, 5 + jnp.where(has_above, 1, 0) + jnp.where(has_below, 1, 0))

    def swap(k, size, w):
        return remote(
            weights[w].at[:, columns(k, size)],
            full.at[w, block_rows(z, 1 - c), columns(k, size)],
            swap_send.at[k, w],
            swap_recv.at[k, w],
            partner,
        )

    def swap_arrival(k, size, w):
        return remote(
            weights[w].at[:, columns(k, size)],
            full.at[w, block_rows(z, c), columns(k, size)],
            swap_send.at[k, w],
            swap_recv.at[k, w],
            partner,
        )

    def own(w):
        return pltpu.make_async_copy(weights[w], full.at[w, block_rows(z, c)], own_sem.at[w])

    def start_swap(k):
        @pl.when(jnp.logical_not(native))
        def _():
            def body(k, size):
                for w in range(WEIGHTS):
                    swap(k, size, w).start()

            each(k, body)

    def token(a, way):
        device, at = ((flip_x, chip), (flip_y, chip), (flip_y, chip_x))[way]
        src = tokens.at[a, slot(chip_x)] if way == 2 else token_refs[a]
        return remote(src, tokens.at[a, slot(at)], token_send.at[a, way], token_recv.at[a, way], device)

    def token_arrival(a, way):
        at = (chip_x, chip_y, chip_both)[way]
        return remote(token_refs[a], tokens.at[a, slot(at)], token_send.at[a, way], token_recv.at[a, way], flip_x)

    def token_home(a):
        return pltpu.make_async_copy(token_refs[a], tokens.at[a, slot(chip)], token_own.at[a])

    @pl.when(native)
    def _():
        for w in range(WEIGHTS):
            own(w).start()

    for a in range(TOKENS_IN):
        token_home(a).start()
    start_swap(0)
    for a in range(TOKENS_IN):
        token(a, 0).start()
        token(a, 1).start()
        if a < TOKENS_IN - 1 and a + 1 < chunks:
            start_swap(a + 1)
    lax.fori_loop(TOKENS_IN, chunks, lambda k, _: (start_swap(k), 0)[1], 0)

    later_acc[...] = jnp.zeros_like(later_acc)
    input_acc[...] = jnp.zeros_like(input_acc)

    @pl.when(native)
    def _():
        for w in range(WEIGHTS):
            own(w).wait()

    def line(k, size, w, block, upward):
        where = full.at[w, block_rows(block, c), columns(k, size)]
        send = (up_send if upward else down_send).at[k, w, block]
        return remote(where, where, send, line_recv.at[k, w, block], above if upward else below)

    def across(k, size, w, block):
        where = full.at[w, block_rows(block, c), columns(k, size)]
        return remote(where, where, pair_send.at[k, w, block], pair_recv.at[k, w, block], pair)

    def across_arrival(k, size, w, block):
        where = full.at[w, block_rows(block, 1 - c), columns(k, size)]
        return remote(where, where, pair_send.at[k, w, block], pair_recv.at[k, w, block], pair)

    def send_own(k):
        def body(k, size):
            for w in range(WEIGHTS):
                @pl.when(jnp.logical_not(native))
                def _():
                    swap_arrival(k, size, w).wait_recv()

                @pl.when(has_above)
                def _():
                    line(k, size, w, z, True).start()

                @pl.when(has_below)
                def _():
                    line(k, size, w, z, False).start()

                across(k, size, w, z).start()

        each(k, body)

    def pass_on(k):
        def body(k, size):
            def step(d, _):
                for w in range(WEIGHTS):
                    @pl.when(z - d >= 0)
                    def _():
                        line(k, size, w, z - d, True).wait_recv()

                        @pl.when(has_above)
                        def _():
                            line(k, size, w, z - d, True).start()

                        across(k, size, w, z - d).start()

                    @pl.when(z + d <= nz - 1)
                    def _():
                        line(k, size, w, z + d, False).wait_recv()

                        @pl.when(has_below)
                        def _():
                            line(k, size, w, z + d, False).start()

                        across(k, size, w, z + d).start()

                return 0

            lax.fori_loop(1, nz, step, 0)

        each(k, body)

    def act(k, size, w):
        return remote(
            acts.at[w, 0, :, columns(k, size)],
            acts.at[w, 1, :, columns(k, size)],
            act_send.at[k, w],
            act_recv.at[k, w],
            pair,
        )

    def turn_ref(a, block):
        return other_tokens.at[a, :, pl.ds(block * depth, depth)]

    def other(a, block):
        return remote(
            tokens.at[a, :, block_rows(block, 1 - c)],
            turn_ref(a, block),
            other_send.at[a, block],
            other_recv.at[a, block],
            pair,
        )

    tiles = half // row_tile
    piece = 512 if model % 512 == 0 else model

    def tile_rows(r):
        return pl.ds(pl.multiple_of(r * row_tile, row_tile), row_tile)

    def by_columns_to(acc, where, pairs, cols):
        def step(n, _):
            out = pl.ds(pl.multiple_of(n * piece, piece), piece)
            value = acc[where, out]
            for left, w in pairs:
                value = value + lax.dot_general(
                    left, full[w, out, cols], (((1,), (1,)), ((), ())), preferred_element_type=jnp.float32
                )
            acc[where, out] = value
            return 0

        lax.fori_loop(0, model // piece, step, 0)

    def earlier(k):
        def body(k, size):
            cols = columns(k, size)

            def wait_block(block, _):
                for w in range(WEIGHTS):
                    across_arrival(k, size, w, block).wait_recv()
                return 0

            lax.fori_loop(0, nz, wait_block, 0)

            def tile(r, _):
                where = tile_rows(r)
                gate = dot(tokens[0, where, :], full[0, :, cols])
                lift = dot(tokens[0, where, :], full[1, :, cols])
                back = dot(tokens[1, where, :], full[2, :, cols])
                active, slope = silu_parts(gate)
                acts[2, 0, where, cols] = (active * lift).astype(jnp.bfloat16)
                gate_back = (back * lift * slope).astype(jnp.bfloat16)
                up_back = (back * active).astype(jnp.bfloat16)
                acts[0, 0, where, cols] = gate_back
                acts[1, 0, where, cols] = up_back
                return 0

            lax.fori_loop(0, tiles, tile, 0)
            for w in range(WEIGHTS):
                act(k, size, w).start()

            def finish(r, _):
                where = tile_rows(r)
                by_columns_to(input_acc, where, ((acts[0, 0, where, cols], 0), (acts[1, 0, where, cols], 1)), cols)
                return 0

            lax.fori_loop(0, tiles, finish, 0)

        each(k, body)

    def later(k):
        def body(k, size):
            cols = columns(k, size)

            def tile(r, _):
                where = tile_rows(r)
                gate = dot(tokens[2, where, :], full[0, :, cols])
                lift = dot(tokens[2, where, :], full[1, :, cols])
                hidden = (jax.nn.silu(gate) * lift).astype(jnp.bfloat16)
                by_columns_to(later_acc, where, ((hidden, 2),), cols)
                return 0

            lax.fori_loop(0, tiles, tile, 0)

        each(k, body)

    def part(o, way):
        device, at = ((flip_x, chip_x), (flip_y, chip_y), (flip_both, chip_both))[way]
        return remote(
            tokens.at[(2, 0)[o], slot(at)], parts_in.at[o, way], part_send.at[o, way], part_recv.at[o, way], device
        )

    def send_parts(o):
        acc = (later_acc, input_acc)[o]

        def step(r, _):
            where = tile_rows(r)
            tokens[(2, 0)[o], where, :] = acc[where, :].astype(jnp.bfloat16)
            return 0

        lax.fori_loop(0, tiles, step, 0)
        for way in (2, 0, 1):
            part(o, way).start()

    def running(k, size, w, index, device):
        where = sums.at[w, index, :, columns(k, size)]
        return remote(where, where, sum_send.at[k, w, index], sum_recv.at[k, w, index], device)

    home = jnp.where(has_above, nz - 1 + z, z - 1)

    def give(k, size, w):
        cols = columns(k, size)
        return remote(sums.at[w, home, :, cols], final.at[w, :, cols], final_send.at[k, w], final_recv.at[k, w], partner)

    def product(k, size, w, target):
        source = 1 if w == 2 else 0
        cols = columns(k, size)
        value = dot(turned[source, target, 0], acts[w, 0, :, cols])
        return value + dot(turned[source, target, 1], acts[w, 1, :, cols])

    def add_arrived(k, size, w, index, device, here):
        running(k, size, w, index, device).wait_recv()
        dots[:, here] += sums[w, index, :, columns(k, size)].astype(jnp.float32)

    def reduce(k):
        def body(k, size):
            here = pl.ds(0, size)
            for w in range(WEIGHTS):
                act(k, size, w).wait_recv()

            def phase(n, _):
                upward = (n == 0) == (2 * z < nz - 1)
                count = jnp.where(upward, nz - 1 - z, z)
                has_previous = jnp.where(upward, z, nz - 1 - z) > 0
                device = (z + jnp.where(upward, 1, -1), x, y, c)

                for w in (2, 0, 1):
                    def send(m, _):
                        target = jnp.where(upward, nz - 1 - m, m)
                        index = jnp.where(upward, target - 1, nz - 1 + target)
                        dots[:, here] = product(k, size, w, target)

                        @pl.when(has_previous)
                        def _():
                            add_arrived(k, size, w, index, device, here)

                        sums[w, index, :, columns(k, size)] = dots[:, here].astype(jnp.bfloat16)
                        running(k, size, w, index, device).start()
                        return 0

                    lax.fori_loop(0, count, send, 0)
                return 0

            lax.fori_loop(0, 2, phase, 0)

        each(k, body)

    def finish_sum(k):
        def body(k, size):
            cols = columns(k, size)
            here = pl.ds(0, size)
            for w in (2, 0, 1):
                dots[:, here] = product(k, size, w, z)

                @pl.when(has_below)
                def _():
                    add_arrived(k, size, w, z - 1, below, here)

                @pl.when(has_above)
                def _():
                    add_arrived(k, size, w, nz - 1 + z, above, here)

                @pl.when(native)
                def _():
                    final[w, :, cols] = dots[:, here].astype(jnp.bfloat16)

                @pl.when(jnp.logical_not(native))
                def _():
                    sums[w, home, :, cols] = dots[:, here].astype(jnp.bfloat16)
                    give(k, size, w).start()

        each(k, body)

    def forward_token(a):
        token_arrival(a, 0).wait_recv()
        token(a, 2).start()

    send_own(0)
    forward_token(0)
    if chunks > 1:
        send_own(1)
    forward_token(1)
    pass_on(0)
    forward_token(2)
    middle = jnp.logical_and(has_above, has_below)
    lead = jnp.where(middle, ahead, 1)
    for k in range(1, min(ahead, chunks)):
        if k > 1:
            send_own(k)

        @pl.when(middle)
        def _():
            pass_on(k)

    for a in range(2):
        token_home(a).wait()
        token_arrival(a, 1).wait_recv()
        token_arrival(a, 2).wait_recv()
        for block in range(nz):
            other(a, block).start()
    for a in range(2):
        for block in range(nz):
            turned[a, block, 0] = tokens[a, :, block_rows(block, c)].T
    for a in range(2):
        for block in range(nz):
            other(a, block).wait()
            turned[a, block, 1] = other_tokens[a, :, block * depth : (block + 1) * depth].T
    for a in range(2):
        for way in range(3):
            token(a, way).wait_send()

    def iteration(i, _):
        @pl.when(jnp.logical_and(i + ahead < chunks, i + ahead >= 2))
        def _():
            send_own(i + ahead)

        @pl.when(i < chunks)
        def _():
            earlier(i)

        @pl.when(i == chunks - 1)
        def _():
            send_parts(1)

        @pl.when(i + lead < chunks)
        def _():
            pass_on(i + lead)

        @pl.when(i == 1)
        def _():
            token_home(2).wait()
            token_arrival(2, 1).wait_recv()
            token_arrival(2, 2).wait_recv()
            for way in range(3):
                token(2, way).wait_send()

        lax.fori_loop(
            jnp.maximum(i - 1, 0), jnp.where(i == chunks - 1, chunks, jnp.where(i < chunks, i, 0)), lambda k, _: (later(k), 0)[1], 0
        )

        @pl.when(i == chunks - 1)
        def _():
            send_parts(0)

        @pl.when(jnp.logical_and(i >= lag, i - lag < chunks))
        def _():
            reduce(i - lag)

        @pl.when(i >= 2)
        def _():
            finish_sum(i - 2)

        return 0

    lag = jnp.where(middle, 1, 0)
    lax.fori_loop(0, chunks + 2, iteration, 0)

    for o, out_ref in ((1, input_grad_ref), (0, later_out_ref)):
        for way in range(3):
            part(o, way).wait()
        mine = slot(chip)
        total = tokens[(2, 0)[o], mine, :].astype(jnp.float32)
        for way in range(3):
            total = total + parts_in[o, way].astype(jnp.float32)
        parts_in[o, 0] = total.astype(jnp.bfloat16)
        pltpu.make_async_copy(parts_in.at[o, 0], out_ref, out_sem.at[o]).start()

    @pl.when(jnp.logical_not(native))
    def _():
        def wait_final(k, _):
            def body(k, size):
                for w in range(WEIGHTS):
                    give(k, size, w).wait()
                    swap(k, size, w).wait_send()

            each(k, body)
            return 0

        lax.fori_loop(0, chunks, wait_final, 0)

    for w, out_ref in enumerate((gate_sum_ref, up_sum_ref, down_sum_ref)):
        pltpu.make_async_copy(final.at[w], out_ref, out_sem.at[2 + w]).start()

    def drain(k, _):
        def body(k, size):
            for w in range(WEIGHTS):
                act(k, size, w).wait_send()

                def block_sends(block, _):
                    across(k, size, w, block).wait_send()

                    @pl.when(jnp.logical_and(has_above, block <= z))
                    def _():
                        line(k, size, w, block, True).wait_send()

                    @pl.when(jnp.logical_and(has_below, block >= z))
                    def _():
                        line(k, size, w, block, False).wait_send()

                    @pl.when(block > z)
                    def _():
                        running(k, size, w, block - 1, above).wait_send()

                    @pl.when(block < z)
                    def _():
                        running(k, size, w, nz - 1 + block, below).wait_send()

                    return 0

                lax.fori_loop(0, nz, block_sends, 0)

        each(k, body)
        return 0

    lax.fori_loop(0, chunks, drain, 0)
    for o, out_ref in ((1, input_grad_ref), (0, later_out_ref)):
        pltpu.make_async_copy(parts_in.at[o, 0], out_ref, out_sem.at[o]).wait()
    for w, out_ref in enumerate((gate_sum_ref, up_sum_ref, down_sum_ref)):
        pltpu.make_async_copy(final.at[w], out_ref, out_sem.at[2 + w]).wait()


def fused(nz, later_rows, earlier_rows, cotangent, gate_weight, up_weight, down_weight):
    rows, model = later_rows.shape
    depth, ff = gate_weight.shape
    half = 4 * rows
    width = 256 if ff > 256 else ff
    chunks = -(-ff // width)
    row_tile = half // 2 if (half // 2) % 16 == 0 else half
    dma = pltpu.SemaphoreType.DMA
    bf16, f32 = jnp.bfloat16, jnp.float32
    scratch = [
        pltpu.VMEM((WEIGHTS, model, ff), bf16),
        pltpu.VMEM((TOKENS_IN, half, model), bf16),
        pltpu.VMEM((2, half, nz * depth), bf16),
        pltpu.VMEM((2, nz, 2, depth, half), bf16),
        pltpu.VMEM((WEIGHTS, 2, half, ff), bf16),
        pltpu.VMEM((WEIGHTS, 2 * (nz - 1), depth, ff), bf16),
        pltpu.VMEM((half, model), f32),
        pltpu.VMEM((half, model), f32),
        pltpu.VMEM((2, 3, rows, model), bf16),
        pltpu.VMEM((WEIGHTS, depth, ff), bf16),
        pltpu.VMEM((depth, width), f32),
        dma((WEIGHTS,)),
        dma((chunks, WEIGHTS)),
        dma((chunks, WEIGHTS)),
        dma((chunks, WEIGHTS, nz)),
        dma((chunks, WEIGHTS, nz)),
        dma((chunks, WEIGHTS, nz)),
        dma((chunks, WEIGHTS, nz)),
        dma((chunks, WEIGHTS, nz)),
        dma((TOKENS_IN,)),
        dma((TOKENS_IN, 3)),
        dma((TOKENS_IN, 3)),
        dma((2, nz)),
        dma((2, nz)),
        dma((chunks, WEIGHTS)),
        dma((chunks, WEIGHTS)),
        dma((chunks, WEIGHTS, 2 * (nz - 1))),
        dma((chunks, WEIGHTS, 2 * (nz - 1))),
        dma((chunks, WEIGHTS)),
        dma((chunks, WEIGHTS)),
        dma((2, 3)),
        dma((2, 3)),
        dma((5,)),
    ]
    return pl.pallas_call(
        functools.partial(fused_kernel, nz, width, 2, row_tile),
        out_shape=[jax.ShapeDtypeStruct((rows, model), bf16)] * 2
        + [jax.ShapeDtypeStruct((depth, ff), bf16)] * 3,
        in_specs=[pl.BlockSpec(memory_space=pl.ANY)] * 6,
        out_specs=[pl.BlockSpec(memory_space=pl.ANY)] * 5,
        scratch_shapes=scratch,
        compiler_params=pltpu.CompilerParams(
            collective_id=0, has_side_effects=True, vmem_limit_bytes=67_000_000
        ),
        cost_estimate=pl.CostEstimate(flops=22 * half * model * ff, bytes_accessed=0, transcendentals=0),
    )(later_rows, earlier_rows, cotangent, gate_weight, up_weight, down_weight)


def general(mesh):
    nf, nt = mesh.shape["fs"], mesh.shape["tp"]
    nx = max(d for d in range(1, nf + 1) if nf % d == 0 and d * d <= nf)
    nz = nf // nx
    split = Mesh(mesh.devices.reshape(nz, nx, nt), ("z", "x", "tp"))
    plane = ("x", "tp")

    def local(
        later_rows,
        earlier_rows,
        cotangent,
        gate_weight,
        up_weight,
        down_weight,
        gate_grad_sum,
        up_grad_sum,
        down_grad_sum,
    ):
        gate_full, gate_last = gather_line(spread_columns(gate_weight, nx), nz)
        up_full, up_last = gather_line(spread_columns(up_weight, nx), nz)
        rows_all = lax.all_gather(earlier_rows, plane, axis=0, tiled=True)
        back_all = lax.all_gather(cotangent, plane, axis=0, tiled=True)
        piece = lax.all_gather(after(later_rows, *gate_last), plane, axis=0, tiled=True)

        gate_e = dot(rows_all, gate_full)
        up_e = dot(rows_all, up_full)
        activation, act_slope = silu_parts(gate_e)
        hidden_e = (activation * up_e).astype(jnp.bfloat16)
        down_parts = by_rows(back_all, hidden_e)
        down_grad, down_first = scatter_line(down_parts, nz)
        later_hidden = (jax.nn.silu(dot(piece, gate_full)) * dot(piece, up_full)).astype(jnp.bfloat16)
        down_block = after(spread_columns(down_weight, nx), *gate_last, *up_last)
        down_full, _ = gather_line(down_block, nz, lambda: ((gate_e, up_e), (down_parts, later_hidden) + down_first))
        later_parts = by_columns(later_hidden, down_full).astype(jnp.bfloat16)
        later_out = lax.psum_scatter(later_parts, plane, scatter_dimension=0, tiled=True)
        back_hidden = dot(back_all, down_full)
        gate_back = (back_hidden * up_e * act_slope).astype(jnp.bfloat16)
        up_back = (back_hidden * activation).astype(jnp.bfloat16)
        gate_parts = by_rows(rows_all, gate_back)
        up_parts = by_rows(rows_all, up_back)
        gate_grad, gate_first = scatter_line(gate_parts, nz)
        up_grad, _ = scatter_line(up_parts, nz)
        gate_back = after(gate_back, *gate_first)
        up_back = after(up_back, *gate_first)
        input_grad = lax.psum_scatter(
            after(
                (by_columns(gate_back, gate_full) + by_columns(up_back, up_full)).astype(jnp.bfloat16),
                later_out,
            ),
            plane,
            scatter_dimension=0,
            tiled=True,
        )
        return (
            later_out,
            input_grad,
            gate_grad_sum + join_columns(gate_grad, nx),
            up_grad_sum + join_columns(up_grad, nx),
            down_grad_sum + join_columns(down_grad, nx),
        )

    rows, weights = P(("z", "x", "tp"), None), P(("z", "x"), "tp")
    return jax.shard_map(
        local,
        mesh=split,
        in_specs=(rows,) * 3 + (weights,) * 6,
        out_specs=(rows,) * 2 + (weights,) * 3,
        check_vma=False,
    )


def solution(mesh):
    nf, nt = mesh.shape["fs"], mesh.shape["tp"]
    nx = max(d for d in range(1, nf + 1) if nf % d == 0 and d * d <= nf)
    nz = nf // nx
    if nx != 2 or nt != 4:
        return general(mesh)
    split = Mesh(mesh.devices.reshape(nz, 2, 2, 2), ("z", "x", "y", "c"))

    def local(later_rows, earlier_rows, cotangent, gate, up, down, *grad_sums):
        later_out, input_grad, *totals = fused(nz, later_rows, earlier_rows, cotangent, gate, up, down)
        return (later_out, input_grad, *(s + t.astype(jnp.float32) for s, t in zip(grad_sums, totals)))

    rows, weights = P(("z", "x", "y", "c"), None), P(("z", "x"), ("y", "c"))
    return jax.shard_map(
        local,
        mesh=split,
        in_specs=(rows,) * 3 + (weights,) * 6,
        out_specs=(rows,) * 2 + (weights,) * 3,
        check_vma=False,
    )
```

```python
import functools

import jax
import jax.numpy as jnp
from jax import lax
from jax.experimental import pallas as pl
from jax.experimental.pallas import tpu as pltpu
from jax.sharding import Mesh, PartitionSpec as P


def silu_parts(gate):
    sigma = jax.nn.sigmoid(gate)
    return (gate * sigma, sigma * (1.0 + gate * (1.0 - sigma)))


def by_columns(left, right):
    return lax.dot_general(
        left, right, (((1,), (1,)), ((), ())), preferred_element_type=jnp.float32
    )


def by_rows(left, right):
    return lax.dot_general(
        left, right, (((0,), (0,)), ((), ())), preferred_element_type=jnp.float32
    )


def dot(left, right):
    return jnp.dot(left, right, preferred_element_type=jnp.float32)


def pick(index, choices):
    value = choices[-1]
    for at in range(len(choices) - 2, -1, -1):
        value = jnp.where(index == at, choices[at], value)
    return value


def shift(value, axis, size, by):
    return lax.ppermute(value, axis, [(i, (i + by) % size) for i in range(size)])


def spread_columns(weight, nx):
    x = lax.axis_index("x")
    rows, columns = weight.shape[0], weight.shape[1] // nx
    parts = [weight[:, c * columns : (c + 1) * columns] for c in range(nx)]
    whole = [pick(x, parts)]
    for by in range(1, nx):
        whole.append(shift(pick((x + by) % nx, parts), "x", nx, by))
    return jnp.concatenate([pick((x - c) % nx, whole) for c in range(nx)], axis=0)


def join_columns(total, nx):
    x = lax.axis_index("x")
    rows = total.shape[0] // nx
    parts = [total[c * rows : (c + 1) * rows] for c in range(nx)]
    whole = [pick(x, parts)]
    for by in range(1, nx):
        sent = pick((x + by) % nx, parts).astype(jnp.bfloat16)
        whole.append(shift(sent, "x", nx, by).astype(jnp.float32))
    return jnp.concatenate([pick((x - c) % nx, whole) for c in range(nx)], axis=1)


def after(value, *earlier):
    return lax.optimization_barrier((value,) + earlier)[0]


def gather_line(block, nz, middle=lambda: ((), ())):
    z = lax.axis_index("z")
    ahead_step, ahead_use = middle()
    up = down = block
    ups, downs = [block], [block]
    for step in range(1, nz):
        if step == nz - 1 and ahead_step:
            up, down = after(up, *ahead_step), after(down, *ahead_step)
        up = lax.ppermute(up, "z", [(i, i + 1) for i in range(step - 1, nz - 1)])
        down = lax.ppermute(down, "z", [(i, i - 1) for i in range(1, nz - step + 1)])
        ups.append(up)
        downs.append(down)
    rows = block.shape[0]
    whole = jnp.zeros((nz * rows, block.shape[1]), block.dtype)
    whole = lax.dynamic_update_slice_in_dim(whole, block, z * rows, 0)
    for back in range(1, nz):
        arrived = jnp.where(z >= back, ups[back], downs[nz - back])
        if ahead_use:
            arrived = after(arrived, *ahead_use)
        whole = lax.dynamic_update_slice_in_dim(whole, arrived, ((z - back) % nz) * rows, 0)
    return whole, (ups[max(nz - 2, 0)], downs[max(nz - 2, 0)])


def scatter_line(parts, nz):
    z = lax.axis_index("z")
    rows = parts.shape[0] // nz

    def block(index):
        return lax.dynamic_slice_in_dim(parts, (index % nz) * rows, rows, 0)

    up = down = None
    first = ()
    for step in range(1, nz):
        up_sum, down_sum = block(z - step), block(z + step)
        if step > 1:
            up_sum = up_sum + up.astype(jnp.float32)
            down_sum = down_sum + down.astype(jnp.float32)
        up = lax.ppermute(
            up_sum.astype(jnp.bfloat16), "z", [(i, i + 1) for i in range(min(step, nz - 1))]
        )
        down = lax.ppermute(
            down_sum.astype(jnp.bfloat16), "z", [(i, i - 1) for i in range(max(nz - step, 1), nz)]
        )
        first = first or (up, down)
    total = block(z)
    if nz > 1:
        total = total + up.astype(jnp.float32) + down.astype(jnp.float32)
    return total, first


MESH = pl.DeviceIdType.MESH
TOKENS_IN = 3
WEIGHTS = 3


def fused_kernel(
    nz,
    width,
    ahead,
    row_tile,
    later_ref,
    earlier_ref,
    cotangent_ref,
    gate_ref,
    up_ref,
    down_ref,
    later_out_ref,
    input_grad_ref,
    gate_sum_ref,
    up_sum_ref,
    down_sum_ref,
    full,
    tokens,
    other_tokens,
    turned,
    acts,
    sums,
    later_acc,
    input_acc,
    parts_in,
    final,
    dots,
    own_sem,
    swap_send,
    swap_recv,
    line_recv,
    pair_recv,
    up_send,
    down_send,
    pair_send,
    token_own,
    token_send,
    token_recv,
    other_send,
    other_recv,
    act_send,
    act_recv,
    sum_send,
    sum_recv,
    final_send,
    final_recv,
    part_send,
    part_recv,
    out_sem,
):
    z, x, y, c = (lax.axis_index(name) for name in ("z", "x", "y", "c"))
    rows = later_ref.shape[0]
    depth, ff = gate_ref.shape
    model = later_ref.shape[1]
    half = tokens.shape[1]
    chunks = -(-ff // width)
    head = ff - (chunks - 1) * width
    pace = 2
    hold = max(chunks - 3, 1)

    above, below = (z + 1, x, y, c), (z - 1, x, y, c)
    pair = (z, x, y, 1 - c)
    flip_x, flip_y, flip_both = (z, 1 - x, y, c), (z, x, 1 - y, c), (z, 1 - x, 1 - y, c)
    partner = (z, 1 - x, y, 1 - c)
    chip = 2 * x + y
    chip_x, chip_y, chip_both = 2 * (1 - x) + y, 2 * x + 1 - y, 2 * (1 - x) + 1 - y
    native = c == x
    has_above, has_below = z < nz - 1, z > 0

    weights = (gate_ref, up_ref, down_ref)
    token_refs = (earlier_ref, cotangent_ref, later_ref)

    def remote(src, dst, send, recv, device):
        return pltpu.make_async_remote_copy(
            src_ref=src, dst_ref=dst, send_sem=send, recv_sem=recv, device_id=device, device_id_type=MESH
        )

    def each(k, body):
        if head == width:
            body(k, width)
            return

        @pl.when(k > 0)
        def _():
            body(k, width)

        @pl.when(k == 0)
        def _():
            body(k, head)

    def columns(k, size):
        return pl.ds(pl.multiple_of(jnp.maximum(k * width - (width - head), 0), 128), size)

    def block_rows(block, parity):
        return pl.ds(pl.multiple_of((block * 2 + parity) * depth, depth), depth)

    def slot(index):
        return pl.ds(pl.multiple_of(index * rows, rows), rows)

    barrier = pltpu.get_barrier_semaphore()
    for device in (pair, flip_x, flip_y, flip_both, partner):
        pl.semaphore_signal(barrier, inc=1, device_id=device, device_id_type=MESH)

    @pl.when(has_above)
    def _():
        pl.semaphore_signal(barrier, inc=1, device_id=above, device_id_type=MESH)

    @pl.when(has_below)
    def _():
        pl.semaphore_signal(barrier, inc=1, device_id=below, device_id_type=MESH)

    pl.semaphore_wait(barrier, 5 + jnp.where(has_above, 1, 0) + jnp.where(has_below, 1, 0))

    def swap(k, size, w):
        return remote(
            weights[w].at[:, columns(k, size)],
            full.at[w, block_rows(z, 1 - c), columns(k, size)],
            swap_send.at[k, w],
            swap_recv.at[k, w],
            partner,
        )

    def swap_arrival(k, size, w):
        return remote(
            weights[w].at[:, columns(k, size)],
            full.at[w, block_rows(z, c), columns(k, size)],
            swap_send.at[k, w],
            swap_recv.at[k, w],
            partner,
        )

    def own(w):
        return pltpu.make_async_copy(weights[w], full.at[w, block_rows(z, c)], own_sem.at[w])

    def start_swap(k):
        @pl.when(jnp.logical_not(native))
        def _():
            def body(k, size):
                for w in range(WEIGHTS):
                    swap(k, size, w).start()

            each(k, body)

    def token(a, way):
        device, at = ((flip_x, chip), (flip_y, chip), (flip_y, chip_x))[way]
        src = tokens.at[a, slot(chip_x)] if way == 2 else token_refs[a]
        return remote(src, tokens.at[a, slot(at)], token_send.at[a, way], token_recv.at[a, way], device)

    def token_arrival(a, way):
        at = (chip_x, chip_y, chip_both)[way]
        return remote(token_refs[a], tokens.at[a, slot(at)], token_send.at[a, way], token_recv.at[a, way], flip_x)

    def token_home(a):
        return pltpu.make_async_copy(token_refs[a], tokens.at[a, slot(chip)], token_own.at[a])

    @pl.when(native)
    def _():
        for w in range(WEIGHTS):
            own(w).start()

    for a in range(TOKENS_IN):
        token_home(a).start()
    start_swap(0)
    for a in range(2):
        token(a, 0).start()
        token(a, 1).start()
    lax.fori_loop(1, chunks, lambda k, _: (start_swap(k), 0)[1], 0)

    later_acc[...] = jnp.zeros_like(later_acc)
    input_acc[...] = jnp.zeros_like(input_acc)

    @pl.when(native)
    def _():
        for w in range(WEIGHTS):
            own(w).wait()

    def line(k, size, w, block, upward):
        where = full.at[w, block_rows(block, c), columns(k, size)]
        send = (up_send if upward else down_send).at[k, w, block]
        return remote(where, where, send, line_recv.at[k, w, block], above if upward else below)

    def across(k, size, w, block):
        where = full.at[w, block_rows(block, c), columns(k, size)]
        return remote(where, where, pair_send.at[k, w, block], pair_recv.at[k, w, block], pair)

    def across_arrival(k, size, w, block):
        where = full.at[w, block_rows(block, 1 - c), columns(k, size)]
        return remote(where, where, pair_send.at[k, w, block], pair_recv.at[k, w, block], pair)

    def send_own(k):
        def body(k, size):
            for w in range(WEIGHTS):
                @pl.when(jnp.logical_not(native))
                def _():
                    swap_arrival(k, size, w).wait_recv()

                @pl.when(has_above)
                def _():
                    line(k, size, w, z, True).start()

                @pl.when(has_below)
                def _():
                    line(k, size, w, z, False).start()

                across(k, size, w, z).start()

        each(k, body)

    def pass_on(k):
        def body(k, size):
            def step(d, _):
                for w in range(WEIGHTS):
                    @pl.when(z - d >= 0)
                    def _():
                        line(k, size, w, z - d, True).wait_recv()

                        @pl.when(has_above)
                        def _():
                            line(k, size, w, z - d, True).start()

                        across(k, size, w, z - d).start()

                    @pl.when(z + d <= nz - 1)
                    def _():
                        line(k, size, w, z + d, False).wait_recv()

                        @pl.when(has_below)
                        def _():
                            line(k, size, w, z + d, False).start()

                        across(k, size, w, z + d).start()

                return 0

            lax.fori_loop(1, nz, step, 0)

        each(k, body)

    def act(k, size, w):
        return remote(
            acts.at[w, 0, :, columns(k, size)],
            acts.at[w, 1, :, columns(k, size)],
            act_send.at[k, w],
            act_recv.at[k, w],
            pair,
        )

    def turn_ref(a, block):
        return other_tokens.at[a, :, pl.ds(block * depth, depth)]

    def other(a, block):
        return remote(
            tokens.at[a, :, block_rows(block, 1 - c)],
            turn_ref(a, block),
            other_send.at[a, block],
            other_recv.at[a, block],
            pair,
        )

    tiles = half // row_tile
    piece = 512 if model % 512 == 0 else model

    def tile_rows(r):
        return pl.ds(pl.multiple_of(r * row_tile, row_tile), row_tile)

    def by_columns_to(acc, where, pairs, cols):
        def step(n, _):
            out = pl.ds(pl.multiple_of(n * piece, piece), piece)
            value = acc[where, out]
            for left, w in pairs:
                value = value + lax.dot_general(
                    left, full[w, out, cols], (((1,), (1,)), ((), ())), preferred_element_type=jnp.float32
                )
            acc[where, out] = value
            return 0

        lax.fori_loop(0, model // piece, step, 0)

    def earlier(k):
        def body(k, size):
            cols = columns(k, size)

            def wait_block(block, _):
                for w in range(WEIGHTS):
                    across_arrival(k, size, w, block).wait_recv()
                return 0

            lax.fori_loop(0, nz, wait_block, 0)

            def tile(r, _):
                where = tile_rows(r)
                gate = dot(tokens[0, where, :], full[0, :, cols])
                lift = dot(tokens[0, where, :], full[1, :, cols])
                back = dot(tokens[1, where, :], full[2, :, cols])
                active, slope = silu_parts(gate)
                acts[2, 0, where, cols] = (active * lift).astype(jnp.bfloat16)
                gate_back = (back * lift * slope).astype(jnp.bfloat16)
                up_back = (back * active).astype(jnp.bfloat16)
                acts[0, 0, where, cols] = gate_back
                acts[1, 0, where, cols] = up_back
                return 0

            lax.fori_loop(0, tiles, tile, 0)
            for w in range(WEIGHTS):
                act(k, size, w).start()

            def finish(r, _):
                where = tile_rows(r)
                by_columns_to(input_acc, where, ((acts[0, 0, where, cols], 0), (acts[1, 0, where, cols], 1)), cols)
                return 0

            lax.fori_loop(0, tiles, finish, 0)

        each(k, body)

    def later(k):
        def body(k, size):
            cols = columns(k, size)

            def tile(r, _):
                where = tile_rows(r)
                gate = dot(tokens[2, where, :], full[0, :, cols])
                lift = dot(tokens[2, where, :], full[1, :, cols])
                hidden = (jax.nn.silu(gate) * lift).astype(jnp.bfloat16)
                by_columns_to(later_acc, where, ((hidden, 2),), cols)
                return 0

            lax.fori_loop(0, tiles, tile, 0)

        each(k, body)

    def part(o, way):
        device, at = ((flip_y, chip_y), (flip_y, chip_both), (flip_x, chip_x))[way]
        return remote(
            tokens.at[(2, 0)[o], slot(at)], parts_in.at[o, way], part_send.at[o, way], part_recv.at[o, way], device
        )

    def combine_parts(o):
        part(o, 1).wait_recv()
        mine = slot(chip_x)
        total = tokens[(2, 0)[o], mine, :].astype(jnp.float32) + parts_in[o, 1].astype(jnp.float32)
        tokens[(2, 0)[o], mine, :] = total.astype(jnp.bfloat16)
        part(o, 2).start()

    def send_parts(o):
        acc = (later_acc, input_acc)[o]

        def step(r, _):
            where = tile_rows(r)
            tokens[(2, 0)[o], where, :] = acc[where, :].astype(jnp.bfloat16)
            return 0

        lax.fori_loop(0, tiles, step, 0)
        for way in (1, 0):
            part(o, way).start()

    def running(k, size, w, index, device):
        where = sums.at[w, index, :, columns(k, size)]
        return remote(where, where, sum_send.at[k, w, index], sum_recv.at[k, w, index], device)

    home = jnp.where(has_above, nz - 1 + z, z - 1)

    def give(k, size, w):
        cols = columns(k, size)
        return remote(sums.at[w, home, :, cols], final.at[w, :, cols], final_send.at[k, w], final_recv.at[k, w], partner)

    def product(k, size, w, target):
        source = 1 if w == 2 else 0
        cols = columns(k, size)
        value = dot(turned[source, target, 0], acts[w, 0, :, cols])
        return value + dot(turned[source, target, 1], acts[w, 1, :, cols])

    def add_arrived(k, size, w, index, device, here):
        running(k, size, w, index, device).wait_recv()
        dots[:, here] += sums[w, index, :, columns(k, size)].astype(jnp.float32)

    def reduce(k, first):
        def body(k, size):
            here = pl.ds(0, size)

            @pl.when(first)
            def _():
                for w in range(WEIGHTS):
                    act(k, size, w).wait_recv()

            def phase():
                upward = first == (2 * z < nz - 1)
                count = jnp.where(upward, nz - 1 - z, z)
                has_previous = jnp.where(upward, z, nz - 1 - z) > 0
                device = (z + jnp.where(upward, 1, -1), x, y, c)

                for w in (2, 0, 1):
                    def send(m, _):
                        target = jnp.where(upward, nz - 1 - m, m)
                        index = jnp.where(upward, target - 1, nz - 1 + target)
                        dots[:, here] = product(k, size, w, target)

                        @pl.when(has_previous)
                        def _():
                            add_arrived(k, size, w, index, device, here)

                        sums[w, index, :, columns(k, size)] = dots[:, here].astype(jnp.bfloat16)
                        running(k, size, w, index, device).start()
                        return 0

                    lax.fori_loop(0, count, send, 0)

            phase()

        each(k, body)

    def finish_sum(k):
        def body(k, size):
            cols = columns(k, size)
            here = pl.ds(0, size)
            for w in (2, 0, 1):
                dots[:, here] = product(k, size, w, z)

                @pl.when(has_below)
                def _():
                    add_arrived(k, size, w, z - 1, below, here)

                @pl.when(has_above)
                def _():
                    add_arrived(k, size, w, nz - 1 + z, above, here)

                @pl.when(native)
                def _():
                    final[w, :, cols] = dots[:, here].astype(jnp.bfloat16)

                @pl.when(jnp.logical_not(native))
                def _():
                    sums[w, home, :, cols] = dots[:, here].astype(jnp.bfloat16)
                    give(k, size, w).start()

        each(k, body)

    def forward_token(a):
        token_arrival(a, 0).wait_recv()
        token(a, 2).start()

    middle = jnp.logical_and(has_above, has_below)
    border = jnp.logical_not(middle)
    foreign = jnp.logical_not(native)
    send_own(0)

    @pl.when(native)
    def _():
        send_own(1)

    forward_token(0)

    @pl.when(middle)
    def _():
        pass_on(0)

    forward_token(1)

    @pl.when(foreign)
    def _():
        send_own(1)

    @pl.when(border)
    def _():
        @pl.when(native)
        def _():
            lax.fori_loop(2, chunks, lambda k, _: (send_own(k), 0)[1], 0)

        pass_on(0)

    token(2, 0).start()
    token(2, 1).start()

    @pl.when(middle)
    def _():
        def step(k, _):
            send_own(k + 1)
            pass_on(k)
            return 0

        lax.fori_loop(1, ahead, step, 0)

    for a in range(2):
        token_home(a).wait()
        token_arrival(a, 1).wait_recv()
        token_arrival(a, 2).wait_recv()
        for block in range(nz):
            other(a, block).start()
    for a in range(2):
        for block in range(nz):
            turned[a, block, 0] = tokens[a, :, block_rows(block, c)].T
    for a in range(2):
        for block in range(nz):
            other(a, block).wait()
            turned[a, block, 1] = other_tokens[a, :, block * depth : (block + 1) * depth].T
    for a in range(2):
        for way in range(3):
            token(a, way).wait_send()

    def span(i):
        return jnp.clip(jnp.minimum(pace * (i - hold), i - 2), 0, chunks)

    def iteration(i, _):
        @pl.when(i < chunks)
        def _():
            earlier(i)

        @pl.when(jnp.logical_and(i == 0, jnp.logical_and(foreign, border)))
        def _():
            lax.fori_loop(2, chunks, lambda k, _: (send_own(k), 0)[1], 0)

        @pl.when(i == chunks - 1)
        def _():
            send_parts(1)

        @pl.when(i == chunks)
        def _():
            combine_parts(1)

        @pl.when(jnp.logical_and(middle, i + ahead < chunks))
        def _():
            @pl.when(i + ahead + 1 < chunks)
            def _():
                send_own(i + ahead + 1)

            pass_on(i + ahead)

        @pl.when(i == 0)
        def _():
            forward_token(2)

        @pl.when(i == 1)
        def _():
            token_home(2).wait()
            token_arrival(2, 1).wait_recv()
            token_arrival(2, 2).wait_recv()
            for way in range(3):
                token(2, way).wait_send()

        lax.fori_loop(
            jnp.maximum(i - 1, 0),
            jnp.where(i == chunks - 1, chunks, jnp.where(i < chunks, i, 0)),
            lambda k, _: (later(k), 0)[1],
            0,
        )

        @pl.when(i == chunks - 1)
        def _():
            send_parts(0)

        near = jnp.where(jnp.logical_and(i >= lag, i - lag < chunks), 1, 0)
        far = jnp.where(middle, span(i), span(i + 1))

        def send_sums(n, _):
            first = n < near
            reduce(jnp.where(first, i - lag, far + n - near), first)
            return 0

        lax.fori_loop(0, near + span(i + 1) - far, send_sums, 0)

        @pl.when(jnp.logical_and(border, i + 1 < chunks))
        def _():
            pass_on(i + 1)

        @pl.when(i == chunks)
        def _():
            combine_parts(0)

        done = jnp.where(middle, jnp.clip(i - late, 0, chunks), span(i - 1))
        ready = jnp.where(middle, jnp.clip(i + 1 - late, 0, chunks), span(i))
        lax.fori_loop(done, ready, lambda k, _: (finish_sum(k), 0)[1], 0)
        return 0

    lag = jnp.where(middle, 1, 0)
    late = 3
    lax.fori_loop(0, chunks + late, iteration, 0)

    for o, out_ref in ((1, input_grad_ref), (0, later_out_ref)):
        part(o, 1).wait_send()
        part(o, 0).wait()
        part(o, 2).wait()
        mine = slot(chip)
        total = tokens[(2, 0)[o], mine, :].astype(jnp.float32)
        for way in (0, 2):
            total = total + parts_in[o, way].astype(jnp.float32)
        parts_in[o, 0] = total.astype(jnp.bfloat16)
        pltpu.make_async_copy(parts_in.at[o, 0], out_ref, out_sem.at[o]).start()

    @pl.when(jnp.logical_not(native))
    def _():
        def wait_final(k, _):
            def body(k, size):
                for w in range(WEIGHTS):
                    give(k, size, w).wait()
                    swap(k, size, w).wait_send()

            each(k, body)
            return 0

        lax.fori_loop(0, chunks, wait_final, 0)

    for w, out_ref in enumerate((gate_sum_ref, up_sum_ref, down_sum_ref)):
        pltpu.make_async_copy(final.at[w], out_ref, out_sem.at[2 + w]).start()

    def drain(k, _):
        def body(k, size):
            for w in range(WEIGHTS):
                act(k, size, w).wait_send()

                def block_sends(block, _):
                    across(k, size, w, block).wait_send()

                    @pl.when(jnp.logical_and(has_above, block <= z))
                    def _():
                        line(k, size, w, block, True).wait_send()

                    @pl.when(jnp.logical_and(has_below, block >= z))
                    def _():
                        line(k, size, w, block, False).wait_send()

                    @pl.when(block > z)
                    def _():
                        running(k, size, w, block - 1, above).wait_send()

                    @pl.when(block < z)
                    def _():
                        running(k, size, w, nz - 1 + block, below).wait_send()

                    return 0

                lax.fori_loop(0, nz, block_sends, 0)

        each(k, body)
        return 0

    lax.fori_loop(0, chunks, drain, 0)
    for o, out_ref in ((1, input_grad_ref), (0, later_out_ref)):
        pltpu.make_async_copy(parts_in.at[o, 0], out_ref, out_sem.at[o]).wait()
    for w, out_ref in enumerate((gate_sum_ref, up_sum_ref, down_sum_ref)):
        pltpu.make_async_copy(final.at[w], out_ref, out_sem.at[2 + w]).wait()


def fused(nz, later_rows, earlier_rows, cotangent, gate_weight, up_weight, down_weight):
    rows, model = later_rows.shape
    depth, ff = gate_weight.shape
    half = 4 * rows
    width = 256 if ff > 256 else ff
    chunks = -(-ff // width)
    row_tile = half // 2 if (half // 2) % 16 == 0 else half
    dma = pltpu.SemaphoreType.DMA
    bf16, f32 = jnp.bfloat16, jnp.float32
    scratch = [
        pltpu.VMEM((WEIGHTS, model, ff), bf16),
        pltpu.VMEM((TOKENS_IN, half, model), bf16),
        pltpu.VMEM((2, half, nz * depth), bf16),
        pltpu.VMEM((2, nz, 2, depth, half), bf16),
        pltpu.VMEM((WEIGHTS, 2, half, ff), bf16),
        pltpu.VMEM((WEIGHTS, 2 * (nz - 1), depth, ff), bf16),
        pltpu.VMEM((half, model), f32),
        pltpu.VMEM((half, model), f32),
        pltpu.VMEM((2, 3, rows, model), bf16),
        pltpu.VMEM((WEIGHTS, depth, ff), bf16),
        pltpu.VMEM((depth, width), f32),
        dma((WEIGHTS,)),
        dma((chunks, WEIGHTS)),
        dma((chunks, WEIGHTS)),
        dma((chunks, WEIGHTS, nz)),
        dma((chunks, WEIGHTS, nz)),
        dma((chunks, WEIGHTS, nz)),
        dma((chunks, WEIGHTS, nz)),
        dma((chunks, WEIGHTS, nz)),
        dma((TOKENS_IN,)),
        dma((TOKENS_IN, 3)),
        dma((TOKENS_IN, 3)),
        dma((2, nz)),
        dma((2, nz)),
        dma((chunks, WEIGHTS)),
        dma((chunks, WEIGHTS)),
        dma((chunks, WEIGHTS, 2 * (nz - 1))),
        dma((chunks, WEIGHTS, 2 * (nz - 1))),
        dma((chunks, WEIGHTS)),
        dma((chunks, WEIGHTS)),
        dma((2, 3)),
        dma((2, 3)),
        dma((5,)),
    ]
    return pl.pallas_call(
        functools.partial(fused_kernel, nz, width, min(4, chunks - 1), row_tile),
        out_shape=[jax.ShapeDtypeStruct((rows, model), bf16)] * 2
        + [jax.ShapeDtypeStruct((depth, ff), bf16)] * 3,
        in_specs=[pl.BlockSpec(memory_space=pl.ANY)] * 6,
        out_specs=[pl.BlockSpec(memory_space=pl.ANY)] * 5,
        scratch_shapes=scratch,
        compiler_params=pltpu.CompilerParams(
            collective_id=0, has_side_effects=True, vmem_limit_bytes=67_000_000
        ),
        cost_estimate=pl.CostEstimate(flops=22 * half * model * ff, bytes_accessed=0, transcendentals=0),
    )(later_rows, earlier_rows, cotangent, gate_weight, up_weight, down_weight)


def general(mesh):
    nf, nt = mesh.shape["fs"], mesh.shape["tp"]
    nx = max(d for d in range(1, nf + 1) if nf % d == 0 and d * d <= nf)
    nz = nf // nx
    split = Mesh(mesh.devices.reshape(nz, nx, nt), ("z", "x", "tp"))
    plane = ("x", "tp")

    def local(
        later_rows,
        earlier_rows,
        cotangent,
        gate_weight,
        up_weight,
        down_weight,
        gate_grad_sum,
        up_grad_sum,
        down_grad_sum,
    ):
        gate_full, gate_last = gather_line(spread_columns(gate_weight, nx), nz)
        up_full, up_last = gather_line(spread_columns(up_weight, nx), nz)
        rows_all = lax.all_gather(earlier_rows, plane, axis=0, tiled=True)
        back_all = lax.all_gather(cotangent, plane, axis=0, tiled=True)
        piece = lax.all_gather(after(later_rows, *gate_last), plane, axis=0, tiled=True)

        gate_e = dot(rows_all, gate_full)
        up_e = dot(rows_all, up_full)
        activation, act_slope = silu_parts(gate_e)
        hidden_e = (activation * up_e).astype(jnp.bfloat16)
        down_parts = by_rows(back_all, hidden_e)
        down_grad, down_first = scatter_line(down_parts, nz)
        later_hidden = (jax.nn.silu(dot(piece, gate_full)) * dot(piece, up_full)).astype(jnp.bfloat16)
        down_block = after(spread_columns(down_weight, nx), *gate_last, *up_last)
        down_full, _ = gather_line(down_block, nz, lambda: ((gate_e, up_e), (down_parts, later_hidden) + down_first))
        later_parts = by_columns(later_hidden, down_full).astype(jnp.bfloat16)
        later_out = lax.psum_scatter(later_parts, plane, scatter_dimension=0, tiled=True)
        back_hidden = dot(back_all, down_full)
        gate_back = (back_hidden * up_e * act_slope).astype(jnp.bfloat16)
        up_back = (back_hidden * activation).astype(jnp.bfloat16)
        gate_parts = by_rows(rows_all, gate_back)
        up_parts = by_rows(rows_all, up_back)
        gate_grad, gate_first = scatter_line(gate_parts, nz)
        up_grad, _ = scatter_line(up_parts, nz)
        gate_back = after(gate_back, *gate_first)
        up_back = after(up_back, *gate_first)
        input_grad = lax.psum_scatter(
            after(
                (by_columns(gate_back, gate_full) + by_columns(up_back, up_full)).astype(jnp.bfloat16),
                later_out,
            ),
            plane,
            scatter_dimension=0,
            tiled=True,
        )
        return (
            later_out,
            input_grad,
            gate_grad_sum + join_columns(gate_grad, nx),
            up_grad_sum + join_columns(up_grad, nx),
            down_grad_sum + join_columns(down_grad, nx),
        )

    rows, weights = P(("z", "x", "tp"), None), P(("z", "x"), "tp")
    return jax.shard_map(
        local,
        mesh=split,
        in_specs=(rows,) * 3 + (weights,) * 6,
        out_specs=(rows,) * 2 + (weights,) * 3,
        check_vma=False,
    )


def solution(mesh):
    nf, nt = mesh.shape["fs"], mesh.shape["tp"]
    nx = max(d for d in range(1, nf + 1) if nf % d == 0 and d * d <= nf)
    nz = nf // nx
    if nx != 2 or nt != 4 or nz < 2:
        return general(mesh)
    split = Mesh(mesh.devices.reshape(nz, 2, 2, 2), ("z", "x", "y", "c"))

    def local(later_rows, earlier_rows, cotangent, gate, up, down, *grad_sums):
        later_out, input_grad, *totals = fused(nz, later_rows, earlier_rows, cotangent, gate, up, down)
        return (later_out, input_grad, *(s + t.astype(jnp.float32) for s, t in zip(grad_sums, totals)))

    rows, weights = P(("z", "x", "y", "c"), None), P(("z", "x"), ("y", "c"))
    return jax.shard_map(
        local,
        mesh=split,
        in_specs=(rows,) * 3 + (weights,) * 6,
        out_specs=(rows,) * 2 + (weights,) * 3,
        check_vma=False,
    )
```

```python
import functools

import jax
import jax.numpy as jnp
from jax import lax
from jax.experimental import pallas as pl
from jax.experimental.pallas import tpu as pltpu
from jax.sharding import Mesh, PartitionSpec as P


def silu_parts(gate):
    sigma = jax.nn.sigmoid(gate)
    return (gate * sigma, sigma * (1.0 + gate * (1.0 - sigma)))


def by_columns(left, right):
    return lax.dot_general(
        left, right, (((1,), (1,)), ((), ())), preferred_element_type=jnp.float32
    )


def by_rows(left, right):
    return lax.dot_general(
        left, right, (((0,), (0,)), ((), ())), preferred_element_type=jnp.float32
    )


def dot(left, right):
    return jnp.dot(left, right, preferred_element_type=jnp.float32)


def pick(index, choices):
    value = choices[-1]
    for at in range(len(choices) - 2, -1, -1):
        value = jnp.where(index == at, choices[at], value)
    return value


def shift(value, axis, size, by):
    return lax.ppermute(value, axis, [(i, (i + by) % size) for i in range(size)])


def spread_columns(weight, nx):
    x = lax.axis_index("x")
    rows, columns = weight.shape[0], weight.shape[1] // nx
    parts = [weight[:, c * columns : (c + 1) * columns] for c in range(nx)]
    whole = [pick(x, parts)]
    for by in range(1, nx):
        whole.append(shift(pick((x + by) % nx, parts), "x", nx, by))
    return jnp.concatenate([pick((x - c) % nx, whole) for c in range(nx)], axis=0)


def join_columns(total, nx):
    x = lax.axis_index("x")
    rows = total.shape[0] // nx
    parts = [total[c * rows : (c + 1) * rows] for c in range(nx)]
    whole = [pick(x, parts)]
    for by in range(1, nx):
        sent = pick((x + by) % nx, parts).astype(jnp.bfloat16)
        whole.append(shift(sent, "x", nx, by).astype(jnp.float32))
    return jnp.concatenate([pick((x - c) % nx, whole) for c in range(nx)], axis=1)


def after(value, *earlier):
    return lax.optimization_barrier((value,) + earlier)[0]


def gather_line(block, nz, middle=lambda: ((), ())):
    z = lax.axis_index("z")
    ahead_step, ahead_use = middle()
    up = down = block
    ups, downs = [block], [block]
    for step in range(1, nz):
        if step == nz - 1 and ahead_step:
            up, down = after(up, *ahead_step), after(down, *ahead_step)
        up = lax.ppermute(up, "z", [(i, i + 1) for i in range(step - 1, nz - 1)])
        down = lax.ppermute(down, "z", [(i, i - 1) for i in range(1, nz - step + 1)])
        ups.append(up)
        downs.append(down)
    rows = block.shape[0]
    whole = jnp.zeros((nz * rows, block.shape[1]), block.dtype)
    whole = lax.dynamic_update_slice_in_dim(whole, block, z * rows, 0)
    for back in range(1, nz):
        arrived = jnp.where(z >= back, ups[back], downs[nz - back])
        if ahead_use:
            arrived = after(arrived, *ahead_use)
        whole = lax.dynamic_update_slice_in_dim(whole, arrived, ((z - back) % nz) * rows, 0)
    return whole, (ups[max(nz - 2, 0)], downs[max(nz - 2, 0)])


def scatter_line(parts, nz):
    z = lax.axis_index("z")
    rows = parts.shape[0] // nz

    def block(index):
        return lax.dynamic_slice_in_dim(parts, (index % nz) * rows, rows, 0)

    up = down = None
    first = ()
    for step in range(1, nz):
        up_sum, down_sum = block(z - step), block(z + step)
        if step > 1:
            up_sum = up_sum + up.astype(jnp.float32)
            down_sum = down_sum + down.astype(jnp.float32)
        up = lax.ppermute(
            up_sum.astype(jnp.bfloat16), "z", [(i, i + 1) for i in range(min(step, nz - 1))]
        )
        down = lax.ppermute(
            down_sum.astype(jnp.bfloat16), "z", [(i, i - 1) for i in range(max(nz - step, 1), nz)]
        )
        first = first or (up, down)
    total = block(z)
    if nz > 1:
        total = total + up.astype(jnp.float32) + down.astype(jnp.float32)
    return total, first


MESH = pl.DeviceIdType.MESH
TOKENS_IN = 3
WEIGHTS = 3


def fused_kernel(
    nz,
    width,
    ahead,
    row_tile,
    later_ref,
    earlier_ref,
    cotangent_ref,
    gate_ref,
    up_ref,
    down_ref,
    later_out_ref,
    input_grad_ref,
    gate_sum_ref,
    up_sum_ref,
    down_sum_ref,
    full,
    tokens,
    other_tokens,
    turned,
    acts,
    sums,
    later_acc,
    input_acc,
    parts_in,
    final,
    dots,
    own_sem,
    swap_send,
    swap_recv,
    line_recv,
    pair_recv,
    up_send,
    down_send,
    pair_send,
    token_own,
    token_send,
    token_recv,
    other_send,
    other_recv,
    act_send,
    act_recv,
    sum_send,
    sum_recv,
    final_send,
    final_recv,
    part_send,
    part_recv,
    out_sem,
):
    z, x, y, c = (lax.axis_index(name) for name in ("z", "x", "y", "c"))
    rows = later_ref.shape[0]
    depth, ff = gate_ref.shape
    model = later_ref.shape[1]
    half = tokens.shape[1]
    chunks = -(-ff // width)
    head = ff - (chunks - 1) * width
    pace = 2
    lead = 1
    hold = max(chunks - 3, 1)

    above, below = (z + 1, x, y, c), (z - 1, x, y, c)
    pair = (z, x, y, 1 - c)
    flip_x, flip_y, flip_both = (z, 1 - x, y, c), (z, x, 1 - y, c), (z, 1 - x, 1 - y, c)
    partner = (z, 1 - x, y, 1 - c)
    chip = 2 * x + y
    chip_x, chip_y, chip_both = 2 * (1 - x) + y, 2 * x + 1 - y, 2 * (1 - x) + 1 - y
    native = c == x
    has_above, has_below = z < nz - 1, z > 0

    weights = (gate_ref, up_ref, down_ref)
    token_refs = (earlier_ref, cotangent_ref, later_ref)

    def remote(src, dst, send, recv, device):
        return pltpu.make_async_remote_copy(
            src_ref=src, dst_ref=dst, send_sem=send, recv_sem=recv, device_id=device, device_id_type=MESH
        )

    def each(k, body):
        if head == width:
            body(k, width)
            return

        @pl.when(k > 0)
        def _():
            body(k, width)

        @pl.when(k == 0)
        def _():
            body(k, head)

    def columns(k, size):
        return pl.ds(pl.multiple_of(jnp.maximum(k * width - (width - head), 0), 128), size)

    def block_rows(block, parity):
        return pl.ds(pl.multiple_of((block * 2 + parity) * depth, depth), depth)

    def slot(index):
        return pl.ds(pl.multiple_of(index * rows, rows), rows)

    barrier = pltpu.get_barrier_semaphore()
    for device in (pair, flip_x, flip_y, flip_both, partner):
        pl.semaphore_signal(barrier, inc=1, device_id=device, device_id_type=MESH)

    @pl.when(has_above)
    def _():
        pl.semaphore_signal(barrier, inc=1, device_id=above, device_id_type=MESH)

    @pl.when(has_below)
    def _():
        pl.semaphore_signal(barrier, inc=1, device_id=below, device_id_type=MESH)

    pl.semaphore_wait(barrier, 5 + jnp.where(has_above, 1, 0) + jnp.where(has_below, 1, 0))

    def swap(k, size, w):
        return remote(
            weights[w].at[:, columns(k, size)],
            full.at[w, block_rows(z, 1 - c), columns(k, size)],
            swap_send.at[w],
            swap_recv.at[k, w],
            partner,
        )

    def swap_arrival(k, size, w):
        return remote(
            weights[w].at[:, columns(k, size)],
            full.at[w, block_rows(z, c), columns(k, size)],
            swap_send.at[w],
            swap_recv.at[k, w],
            partner,
        )

    def own(w):
        return pltpu.make_async_copy(weights[w], full.at[w, block_rows(z, c)], own_sem.at[w])

    def start_swap(k):
        @pl.when(jnp.logical_not(native))
        def _():
            def body(k, size):
                for w in range(WEIGHTS):
                    swap(k, size, w).start()

            each(k, body)

    def token(a, way):
        device, at = ((flip_x, chip), (flip_y, chip), (flip_y, chip_x))[way]
        src = tokens.at[a, slot(chip_x)] if way == 2 else token_refs[a]
        return remote(src, tokens.at[a, slot(at)], token_send.at[a, way], token_recv.at[a, way], device)

    def token_arrival(a, way):
        at = (chip_x, chip_y, chip_both)[way]
        return remote(token_refs[a], tokens.at[a, slot(at)], token_send.at[a, way], token_recv.at[a, way], flip_x)

    def token_home(a):
        return pltpu.make_async_copy(token_refs[a], tokens.at[a, slot(chip)], token_own.at[a])

    @pl.when(native)
    def _():
        for w in range(WEIGHTS):
            own(w).start()

    for a in range(TOKENS_IN):
        token_home(a).start()
    start_swap(0)
    for a in range(2):
        token(a, 0).start()
        token(a, 1).start()
    lax.fori_loop(1, chunks, lambda k, _: (start_swap(k), 0)[1], 0)

    later_acc[...] = jnp.zeros_like(later_acc)
    input_acc[...] = jnp.zeros_like(input_acc)

    @pl.when(native)
    def _():
        for w in range(WEIGHTS):
            own(w).wait()

    def line(k, size, w, block, upward):
        where = full.at[w, block_rows(block, c), columns(k, size)]
        send = (up_send if upward else down_send).at[w, block]
        return remote(where, where, send, line_recv.at[k, w, block], above if upward else below)

    def across(k, size, w, block):
        where = full.at[w, block_rows(block, c), columns(k, size)]
        return remote(where, where, pair_send.at[w, block], pair_recv.at[k, w, block], pair)

    def across_arrival(k, size, w, block):
        where = full.at[w, block_rows(block, 1 - c), columns(k, size)]
        return remote(where, where, pair_send.at[w, block], pair_recv.at[k, w, block], pair)

    def send_own(k):
        def body(k, size):
            for w in range(WEIGHTS):
                @pl.when(jnp.logical_not(native))
                def _():
                    swap_arrival(k, size, w).wait_recv()

                @pl.when(has_above)
                def _():
                    line(k, size, w, z, True).start()

                @pl.when(has_below)
                def _():
                    line(k, size, w, z, False).start()

                across(k, size, w, z).start()

        each(k, body)

    def pass_on(k):
        def body(k, size):
            def step(d, _):
                for w in range(WEIGHTS):
                    @pl.when(z - d >= 0)
                    def _():
                        line(k, size, w, z - d, True).wait_recv()

                        @pl.when(has_above)
                        def _():
                            line(k, size, w, z - d, True).start()

                        across(k, size, w, z - d).start()

                    @pl.when(z + d <= nz - 1)
                    def _():
                        line(k, size, w, z + d, False).wait_recv()

                        @pl.when(has_below)
                        def _():
                            line(k, size, w, z + d, False).start()

                        across(k, size, w, z + d).start()

                return 0

            lax.fori_loop(1, nz, step, 0)

        each(k, body)

    def act(k, size, w):
        return remote(
            acts.at[w, 0, :, columns(k, size)],
            acts.at[w, 1, :, columns(k, size)],
            act_send.at[w],
            act_recv.at[k, w],
            pair,
        )

    def turn_ref(a, block):
        return other_tokens.at[a, :, pl.ds(block * depth, depth)]

    def other(a, block):
        return remote(
            tokens.at[a, :, block_rows(block, 1 - c)],
            turn_ref(a, block),
            other_send.at[a, block],
            other_recv.at[a, block],
            pair,
        )

    tiles = half // row_tile
    piece = 512 if model % 512 == 0 else model

    def tile_rows(r):
        return pl.ds(pl.multiple_of(r * row_tile, row_tile), row_tile)

    def by_columns_to(acc, where, pairs, cols):
        def step(n, _):
            out = pl.ds(pl.multiple_of(n * piece, piece), piece)
            value = acc[where, out]
            for left, w in pairs:
                value = value + lax.dot_general(
                    left, full[w, out, cols], (((1,), (1,)), ((), ())), preferred_element_type=jnp.float32
                )
            acc[where, out] = value
            return 0

        lax.fori_loop(0, model // piece, step, 0)

    def earlier(k):
        def body(k, size):
            cols = columns(k, size)

            def wait_block(block, _):
                for w in range(WEIGHTS):
                    across_arrival(k, size, w, block).wait_recv()
                return 0

            lax.fori_loop(0, nz, wait_block, 0)

            def tile(r, _):
                where = tile_rows(r)
                gate = dot(tokens[0, where, :], full[0, :, cols])
                lift = dot(tokens[0, where, :], full[1, :, cols])
                back = dot(tokens[1, where, :], full[2, :, cols])
                active, slope = silu_parts(gate)
                acts[2, 0, where, cols] = (active * lift).astype(jnp.bfloat16)
                gate_back = (back * lift * slope).astype(jnp.bfloat16)
                up_back = (back * active).astype(jnp.bfloat16)
                acts[0, 0, where, cols] = gate_back
                acts[1, 0, where, cols] = up_back
                return 0

            lax.fori_loop(0, tiles, tile, 0)
            for w in range(WEIGHTS):
                act(k, size, w).start()

            def finish(r, _):
                where = tile_rows(r)
                by_columns_to(input_acc, where, ((acts[0, 0, where, cols], 0), (acts[1, 0, where, cols], 1)), cols)
                return 0

            lax.fori_loop(0, tiles, finish, 0)

        each(k, body)

    def later(k):
        def body(k, size):
            cols = columns(k, size)

            def tile(r, _):
                where = tile_rows(r)
                gate = dot(tokens[2, where, :], full[0, :, cols])
                lift = dot(tokens[2, where, :], full[1, :, cols])
                hidden = (jax.nn.silu(gate) * lift).astype(jnp.bfloat16)
                by_columns_to(later_acc, where, ((hidden, 2),), cols)
                return 0

            lax.fori_loop(0, tiles, tile, 0)

        each(k, body)

    def part(o, way):
        device, at = ((flip_y, chip_y), (flip_y, chip_both), (flip_x, chip_x))[way]
        return remote(
            tokens.at[(2, 0)[o], slot(at)], parts_in.at[o, way], part_send.at[o, way], part_recv.at[o, way], device
        )

    def combine_parts(o):
        part(o, 1).wait_recv()
        mine = slot(chip_x)
        total = tokens[(2, 0)[o], mine, :].astype(jnp.float32) + parts_in[o, 1].astype(jnp.float32)
        tokens[(2, 0)[o], mine, :] = total.astype(jnp.bfloat16)
        part(o, 2).start()

    def send_parts(o):
        acc = (later_acc, input_acc)[o]

        def step(r, _):
            where = tile_rows(r)
            tokens[(2, 0)[o], where, :] = acc[where, :].astype(jnp.bfloat16)
            return 0

        lax.fori_loop(0, tiles, step, 0)
        for way in (1, 0):
            part(o, way).start()

    def running(k, size, w, index, device):
        where = sums.at[w, index, :, columns(k, size)]
        return remote(where, where, sum_send.at[w, index], sum_recv.at[k, w, index], device)

    home = jnp.where(has_above, nz - 1 + z, z - 1)

    def give(k, size, w):
        cols = columns(k, size)
        return remote(sums.at[w, home, :, cols], final.at[w, :, cols], final_send.at[w], final_recv.at[w], partner)

    def product(k, size, w, target):
        source = 1 if w == 2 else 0
        cols = columns(k, size)
        value = dot(turned[source, target, 0], acts[w, 0, :, cols])
        return value + dot(turned[source, target, 1], acts[w, 1, :, cols])

    def add_arrived(k, size, w, index, device, here):
        running(k, size, w, index, device).wait_recv()
        dots[:, here] += sums[w, index, :, columns(k, size)].astype(jnp.float32)

    def reduce(k, first):
        def body(k, size):
            here = pl.ds(0, size)

            @pl.when(first)
            def _():
                for w in range(WEIGHTS):
                    act(k, size, w).wait_recv()

            def phase():
                upward = first == (2 * z < nz - 1)
                count = jnp.where(upward, nz - 1 - z, z)
                has_previous = jnp.where(upward, z, nz - 1 - z) > 0
                device = (z + jnp.where(upward, 1, -1), x, y, c)

                def send(m, _):
                    target = jnp.where(upward, nz - 1 - m, m)
                    index = jnp.where(upward, target - 1, nz - 1 + target)
                    for w in (2, 0, 1):
                        dots[:, here] = product(k, size, w, target)

                        @pl.when(has_previous)
                        def _():
                            add_arrived(k, size, w, index, device, here)

                        sums[w, index, :, columns(k, size)] = dots[:, here].astype(jnp.bfloat16)
                        running(k, size, w, index, device).start()
                    return 0

                lax.fori_loop(0, count, send, 0)

            phase()

        each(k, body)

    def finish_sum(k):
        def body(k, size):
            cols = columns(k, size)
            here = pl.ds(0, size)
            for w in (2, 0, 1):
                dots[:, here] = product(k, size, w, z)

                @pl.when(has_below)
                def _():
                    add_arrived(k, size, w, z - 1, below, here)

                @pl.when(has_above)
                def _():
                    add_arrived(k, size, w, nz - 1 + z, above, here)

                @pl.when(native)
                def _():
                    final[w, :, cols] = dots[:, here].astype(jnp.bfloat16)

                @pl.when(jnp.logical_not(native))
                def _():
                    sums[w, home, :, cols] = dots[:, here].astype(jnp.bfloat16)
                    give(k, size, w).start()

        each(k, body)

    def forward_token(a):
        token_arrival(a, 0).wait_recv()
        token(a, 2).start()

    middle = jnp.logical_and(has_above, has_below)
    border = jnp.logical_not(middle)
    foreign = jnp.logical_not(native)
    send_own(0)

    @pl.when(native)
    def _():
        send_own(1)

    forward_token(0)

    @pl.when(middle)
    def _():
        pass_on(0)

    forward_token(1)

    @pl.when(foreign)
    def _():
        send_own(1)

    @pl.when(border)
    def _():
        @pl.when(native)
        def _():
            lax.fori_loop(2, chunks, lambda k, _: (send_own(k), 0)[1], 0)

        pass_on(0)

        @pl.when(foreign)
        def _():
            lax.fori_loop(2, min(2 + 2, chunks), lambda k, _: (send_own(k), 0)[1], 0)

    token(2, 0).start()
    token(2, 1).start()

    @pl.when(middle)
    def _():
        lax.fori_loop(2, min(1 + lead, chunks), lambda k, _: (send_own(k), 0)[1], 0)

        def step(k, _):
            @pl.when(k + lead < chunks)
            def _():
                send_own(k + lead)

            pass_on(k)
            return 0

        lax.fori_loop(1, ahead, step, 0)

    for a in range(2):
        token_home(a).wait()
        token_arrival(a, 1).wait_recv()
        token_arrival(a, 2).wait_recv()
        for block in range(nz):
            other(a, block).start()
    for a in range(2):
        for block in range(nz):
            turned[a, block, 0] = tokens[a, :, block_rows(block, c)].T
    for a in range(2):
        for block in range(nz):
            other(a, block).wait()
            turned[a, block, 1] = other_tokens[a, :, block * depth : (block + 1) * depth].T
    for a in range(2):
        for way in range(3):
            token(a, way).wait_send()

    def span(i):
        return jnp.clip(jnp.minimum(pace * (i - hold), i - 2), 0, chunks)

    def iteration(i, _):
        @pl.when(i < chunks)
        def _():
            earlier(i)

        @pl.when(jnp.logical_and(i == 0, jnp.logical_and(foreign, border)))
        def _():
            lax.fori_loop(min(2 + 2, chunks), chunks, lambda k, _: (send_own(k), 0)[1], 0)

        @pl.when(i == chunks - 1)
        def _():
            send_parts(1)

        @pl.when(i == chunks)
        def _():
            combine_parts(1)

        @pl.when(jnp.logical_and(middle, i + ahead < chunks))
        def _():
            @pl.when(i + ahead + lead < chunks)
            def _():
                send_own(i + ahead + lead)

            pass_on(i + ahead)

        @pl.when(i == 1)
        def _():
            token_home(2).wait()
            token_arrival(2, 1).wait_recv()
            token_arrival(2, 2).wait_recv()
            for way in range(3):
                token(2, way).wait_send()

        lax.fori_loop(
            jnp.maximum(i - 1, 0),
            jnp.where(i == chunks - 1, chunks, jnp.where(i < chunks, i, 0)),
            lambda k, _: (later(k), 0)[1],
            0,
        )

        @pl.when(i == chunks - 1)
        def _():
            send_parts(0)

        near = jnp.where(jnp.logical_and(i >= lag, i - lag < chunks), 1, 0)
        far = jnp.where(middle, span(i), span(i + 1))

        def send_sums(n, _):
            first = n < near
            reduce(jnp.where(first, i - lag, far + n - near), first)
            return 0

        lax.fori_loop(0, near + span(i + 1) - far, send_sums, 0)

        @pl.when(i == 0)
        def _():
            forward_token(2)

        @pl.when(jnp.logical_and(border, i + 1 < chunks))
        def _():
            pass_on(i + 1)

        @pl.when(i == chunks)
        def _():
            combine_parts(0)

        done = jnp.where(middle, jnp.clip(i - late, 0, chunks), jnp.where(i < chunks, 0, span(i - 1)))
        ready = jnp.where(middle, jnp.clip(i + 1 - late, 0, chunks), jnp.where(i + 1 < chunks, 0, span(i)))
        lax.fori_loop(done, ready, lambda k, _: (finish_sum(k), 0)[1], 0)
        return 0

    lag = jnp.where(middle, 1, 0)
    late = 3
    lax.fori_loop(0, chunks + late, iteration, 0)

    for o, out_ref in ((1, input_grad_ref), (0, later_out_ref)):
        part(o, 1).wait_send()
        part(o, 0).wait()
        part(o, 2).wait()
        mine = slot(chip)
        total = tokens[(2, 0)[o], mine, :].astype(jnp.float32)
        for way in (0, 2):
            total = total + parts_in[o, way].astype(jnp.float32)
        parts_in[o, 0] = total.astype(jnp.bfloat16)
        pltpu.make_async_copy(parts_in.at[o, 0], out_ref, out_sem.at[o]).start()

    @pl.when(foreign)
    def _():
        for w in range(WEIGHTS):
            whole = remote(sums.at[w, home], final.at[w], final_send.at[w], final_recv.at[w], partner)
            whole.wait_send()
            whole.wait_recv()

    for w, out_ref in enumerate((gate_sum_ref, up_sum_ref, down_sum_ref)):
        pltpu.make_async_copy(final.at[w], out_ref, out_sem.at[2 + w]).start()

    for w in range(WEIGHTS):
        remote(acts.at[w, 0], acts.at[w, 1], act_send.at[w], act_recv.at[0, w], pair).wait_send()

        @pl.when(foreign)
        def _():
            remote(
                weights[w], full.at[w, block_rows(z, 1 - c)], swap_send.at[w], swap_recv.at[0, w], partner
            ).wait_send()

        def block_sends(block, _):
            where = full.at[w, block_rows(block, c)]
            remote(where, where, pair_send.at[w, block], pair_recv.at[0, w, block], pair).wait_send()

            @pl.when(jnp.logical_and(has_above, block <= z))
            def _():
                remote(where, where, up_send.at[w, block], line_recv.at[0, w, block], above).wait_send()

            @pl.when(jnp.logical_and(has_below, block >= z))
            def _():
                remote(where, where, down_send.at[w, block], line_recv.at[0, w, block], below).wait_send()

            @pl.when(block != z)
            def _():
                index = jnp.where(block > z, block - 1, nz - 1 + block)
                where = sums.at[w, index]
                device = (z + jnp.where(block > z, 1, -1), x, y, c)
                remote(where, where, sum_send.at[w, index], sum_recv.at[0, w, index], device).wait_send()

            return 0

        lax.fori_loop(0, nz, block_sends, 0)

    for o, out_ref in ((1, input_grad_ref), (0, later_out_ref)):
        pltpu.make_async_copy(parts_in.at[o, 0], out_ref, out_sem.at[o]).wait()
    for w, out_ref in enumerate((gate_sum_ref, up_sum_ref, down_sum_ref)):
        pltpu.make_async_copy(final.at[w], out_ref, out_sem.at[2 + w]).wait()


def fused(nz, later_rows, earlier_rows, cotangent, gate_weight, up_weight, down_weight):
    rows, model = later_rows.shape
    depth, ff = gate_weight.shape
    half = 4 * rows
    width = 256 if ff > 256 else ff
    chunks = -(-ff // width)
    row_tile = half // 2 if (half // 2) % 16 == 0 else half
    dma = pltpu.SemaphoreType.DMA
    bf16, f32 = jnp.bfloat16, jnp.float32
    scratch = [
        pltpu.VMEM((WEIGHTS, model, ff), bf16),
        pltpu.VMEM((TOKENS_IN, half, model), bf16),
        pltpu.VMEM((2, half, nz * depth), bf16),
        pltpu.VMEM((2, nz, 2, depth, half), bf16),
        pltpu.VMEM((WEIGHTS, 2, half, ff), bf16),
        pltpu.VMEM((WEIGHTS, 2 * (nz - 1), depth, ff), bf16),
        pltpu.VMEM((half, model), f32),
        pltpu.VMEM((half, model), f32),
        pltpu.VMEM((2, 3, rows, model), bf16),
        pltpu.VMEM((WEIGHTS, depth, ff), bf16),
        pltpu.VMEM((depth, width), f32),
        dma((WEIGHTS,)),
        dma((WEIGHTS,)),
        dma((chunks, WEIGHTS)),
        dma((chunks, WEIGHTS, nz)),
        dma((chunks, WEIGHTS, nz)),
        dma((WEIGHTS, nz)),
        dma((WEIGHTS, nz)),
        dma((WEIGHTS, nz)),
        dma((TOKENS_IN,)),
        dma((TOKENS_IN, 3)),
        dma((TOKENS_IN, 3)),
        dma((2, nz)),
        dma((2, nz)),
        dma((WEIGHTS,)),
        dma((chunks, WEIGHTS)),
        dma((WEIGHTS, 2 * (nz - 1))),
        dma((chunks, WEIGHTS, 2 * (nz - 1))),
        dma((WEIGHTS,)),
        dma((WEIGHTS,)),
        dma((2, 3)),
        dma((2, 3)),
        dma((5,)),
    ]
    return pl.pallas_call(
        functools.partial(fused_kernel, nz, width, min(4, chunks - 1), row_tile),
        out_shape=[jax.ShapeDtypeStruct((rows, model), bf16)] * 2
        + [jax.ShapeDtypeStruct((depth, ff), bf16)] * 3,
        in_specs=[pl.BlockSpec(memory_space=pl.ANY)] * 6,
        out_specs=[pl.BlockSpec(memory_space=pl.ANY)] * 5,
        scratch_shapes=scratch,
        compiler_params=pltpu.CompilerParams(
            collective_id=0, has_side_effects=True, vmem_limit_bytes=67_000_000
        ),
        cost_estimate=pl.CostEstimate(flops=22 * half * model * ff, bytes_accessed=0, transcendentals=0),
    )(later_rows, earlier_rows, cotangent, gate_weight, up_weight, down_weight)


def general(mesh):
    nf, nt = mesh.shape["fs"], mesh.shape["tp"]
    nx = max(d for d in range(1, nf + 1) if nf % d == 0 and d * d <= nf)
    nz = nf // nx
    split = Mesh(mesh.devices.reshape(nz, nx, nt), ("z", "x", "tp"))
    plane = ("x", "tp")

    def local(
        later_rows,
        earlier_rows,
        cotangent,
        gate_weight,
        up_weight,
        down_weight,
        gate_grad_sum,
        up_grad_sum,
        down_grad_sum,
    ):
        gate_full, gate_last = gather_line(spread_columns(gate_weight, nx), nz)
        up_full, up_last = gather_line(spread_columns(up_weight, nx), nz)
        rows_all = lax.all_gather(earlier_rows, plane, axis=0, tiled=True)
        back_all = lax.all_gather(cotangent, plane, axis=0, tiled=True)
        piece = lax.all_gather(after(later_rows, *gate_last), plane, axis=0, tiled=True)

        gate_e = dot(rows_all, gate_full)
        up_e = dot(rows_all, up_full)
        activation, act_slope = silu_parts(gate_e)
        hidden_e = (activation * up_e).astype(jnp.bfloat16)
        down_parts = by_rows(back_all, hidden_e)
        down_grad, down_first = scatter_line(down_parts, nz)
        later_hidden = (jax.nn.silu(dot(piece, gate_full)) * dot(piece, up_full)).astype(jnp.bfloat16)
        down_block = after(spread_columns(down_weight, nx), *gate_last, *up_last)
        down_full, _ = gather_line(down_block, nz, lambda: ((gate_e, up_e), (down_parts, later_hidden) + down_first))
        later_parts = by_columns(later_hidden, down_full).astype(jnp.bfloat16)
        later_out = lax.psum_scatter(later_parts, plane, scatter_dimension=0, tiled=True)
        back_hidden = dot(back_all, down_full)
        gate_back = (back_hidden * up_e * act_slope).astype(jnp.bfloat16)
        up_back = (back_hidden * activation).astype(jnp.bfloat16)
        gate_parts = by_rows(rows_all, gate_back)
        up_parts = by_rows(rows_all, up_back)
        gate_grad, gate_first = scatter_line(gate_parts, nz)
        up_grad, _ = scatter_line(up_parts, nz)
        gate_back = after(gate_back, *gate_first)
        up_back = after(up_back, *gate_first)
        input_grad = lax.psum_scatter(
            after(
                (by_columns(gate_back, gate_full) + by_columns(up_back, up_full)).astype(jnp.bfloat16),
                later_out,
            ),
            plane,
            scatter_dimension=0,
            tiled=True,
        )
        return (
            later_out,
            input_grad,
            gate_grad_sum + join_columns(gate_grad, nx),
            up_grad_sum + join_columns(up_grad, nx),
            down_grad_sum + join_columns(down_grad, nx),
        )

    rows, weights = P(("z", "x", "tp"), None), P(("z", "x"), "tp")
    return jax.shard_map(
        local,
        mesh=split,
        in_specs=(rows,) * 3 + (weights,) * 6,
        out_specs=(rows,) * 2 + (weights,) * 3,
        check_vma=False,
    )


def solution(mesh):
    nf, nt = mesh.shape["fs"], mesh.shape["tp"]
    nx = max(d for d in range(1, nf + 1) if nf % d == 0 and d * d <= nf)
    nz = nf // nx
    if nx != 2 or nt != 4 or nz < 2:
        return general(mesh)
    split = Mesh(mesh.devices.reshape(nz, 2, 2, 2), ("z", "x", "y", "c"))

    def local(later_rows, earlier_rows, cotangent, gate, up, down, *grad_sums):
        later_out, input_grad, *totals = fused(nz, later_rows, earlier_rows, cotangent, gate, up, down)
        return (later_out, input_grad, *(s + t.astype(jnp.float32) for s, t in zip(grad_sums, totals)))

    rows, weights = P(("z", "x", "y", "c"), None), P(("z", "x"), ("y", "c"))
    return jax.shard_map(
        local,
        mesh=split,
        in_specs=(rows,) * 3 + (weights,) * 6,
        out_specs=(rows,) * 2 + (weights,) * 3,
        check_vma=False,
    )
```

```python
import functools

import jax
import jax.numpy as jnp
from jax import lax
from jax.experimental import pallas as pl
from jax.experimental.pallas import tpu as pltpu
from jax.sharding import Mesh, PartitionSpec as P


def silu_parts(gate):
    sigma = jax.nn.sigmoid(gate)
    return (gate * sigma, sigma * (1.0 + gate * (1.0 - sigma)))


def by_columns(left, right):
    return lax.dot_general(
        left, right, (((1,), (1,)), ((), ())), preferred_element_type=jnp.float32
    )


def by_rows(left, right):
    return lax.dot_general(
        left, right, (((0,), (0,)), ((), ())), preferred_element_type=jnp.float32
    )


def dot(left, right):
    return jnp.dot(left, right, preferred_element_type=jnp.float32)


def pick(index, choices):
    value = choices[-1]
    for at in range(len(choices) - 2, -1, -1):
        value = jnp.where(index == at, choices[at], value)
    return value


def shift(value, axis, size, by):
    return lax.ppermute(value, axis, [(i, (i + by) % size) for i in range(size)])


def spread_columns(weight, nx):
    x = lax.axis_index("x")
    rows, columns = weight.shape[0], weight.shape[1] // nx
    parts = [weight[:, c * columns : (c + 1) * columns] for c in range(nx)]
    whole = [pick(x, parts)]
    for by in range(1, nx):
        whole.append(shift(pick((x + by) % nx, parts), "x", nx, by))
    return jnp.concatenate([pick((x - c) % nx, whole) for c in range(nx)], axis=0)


def join_columns(total, nx):
    x = lax.axis_index("x")
    rows = total.shape[0] // nx
    parts = [total[c * rows : (c + 1) * rows] for c in range(nx)]
    whole = [pick(x, parts)]
    for by in range(1, nx):
        sent = pick((x + by) % nx, parts).astype(jnp.bfloat16)
        whole.append(shift(sent, "x", nx, by).astype(jnp.float32))
    return jnp.concatenate([pick((x - c) % nx, whole) for c in range(nx)], axis=1)


def after(value, *earlier):
    return lax.optimization_barrier((value,) + earlier)[0]


def gather_line(block, nz, middle=lambda: ((), ())):
    z = lax.axis_index("z")
    ahead_step, ahead_use = middle()
    up = down = block
    ups, downs = [block], [block]
    for step in range(1, nz):
        if step == nz - 1 and ahead_step:
            up, down = after(up, *ahead_step), after(down, *ahead_step)
        up = lax.ppermute(up, "z", [(i, i + 1) for i in range(step - 1, nz - 1)])
        down = lax.ppermute(down, "z", [(i, i - 1) for i in range(1, nz - step + 1)])
        ups.append(up)
        downs.append(down)
    rows = block.shape[0]
    whole = jnp.zeros((nz * rows, block.shape[1]), block.dtype)
    whole = lax.dynamic_update_slice_in_dim(whole, block, z * rows, 0)
    for back in range(1, nz):
        arrived = jnp.where(z >= back, ups[back], downs[nz - back])
        if ahead_use:
            arrived = after(arrived, *ahead_use)
        whole = lax.dynamic_update_slice_in_dim(whole, arrived, ((z - back) % nz) * rows, 0)
    return whole, (ups[max(nz - 2, 0)], downs[max(nz - 2, 0)])


def scatter_line(parts, nz):
    z = lax.axis_index("z")
    rows = parts.shape[0] // nz

    def block(index):
        return lax.dynamic_slice_in_dim(parts, (index % nz) * rows, rows, 0)

    up = down = None
    first = ()
    for step in range(1, nz):
        up_sum, down_sum = block(z - step), block(z + step)
        if step > 1:
            up_sum = up_sum + up.astype(jnp.float32)
            down_sum = down_sum + down.astype(jnp.float32)
        up = lax.ppermute(
            up_sum.astype(jnp.bfloat16), "z", [(i, i + 1) for i in range(min(step, nz - 1))]
        )
        down = lax.ppermute(
            down_sum.astype(jnp.bfloat16), "z", [(i, i - 1) for i in range(max(nz - step, 1), nz)]
        )
        first = first or (up, down)
    total = block(z)
    if nz > 1:
        total = total + up.astype(jnp.float32) + down.astype(jnp.float32)
    return total, first


MESH = pl.DeviceIdType.MESH
TOKENS_IN = 3
WEIGHTS = 3


def fused_kernel(
    nz,
    width,
    ahead,
    row_tile,
    later_ref,
    earlier_ref,
    cotangent_ref,
    gate_ref,
    up_ref,
    down_ref,
    later_out_ref,
    input_grad_ref,
    gate_sum_ref,
    up_sum_ref,
    down_sum_ref,
    full,
    tokens,
    other_tokens,
    turned,
    acts,
    sums,
    later_acc,
    input_acc,
    parts_in,
    final,
    dots,
    own_sem,
    swap_send,
    swap_recv,
    line_recv,
    pair_recv,
    up_send,
    down_send,
    pair_send,
    token_own,
    token_send,
    token_recv,
    other_send,
    other_recv,
    act_send,
    act_recv,
    sum_send,
    sum_recv,
    final_send,
    final_recv,
    part_send,
    part_recv,
    out_sem,
):
    z, x, y, c = (lax.axis_index(name) for name in ("z", "x", "y", "c"))
    rows = later_ref.shape[0]
    depth, ff = gate_ref.shape
    model = later_ref.shape[1]
    half = tokens.shape[1]
    chunks = -(-ff // width)
    head = ff - (chunks - 1) * width
    pace = 2
    lead = 1
    hold = max(chunks - 3, 1)

    above, below = (z + 1, x, y, c), (z - 1, x, y, c)
    pair = (z, x, y, 1 - c)
    flip_x, flip_y, flip_both = (z, 1 - x, y, c), (z, x, 1 - y, c), (z, 1 - x, 1 - y, c)
    partner = (z, 1 - x, y, 1 - c)
    chip = 2 * x + y
    chip_x, chip_y, chip_both = 2 * (1 - x) + y, 2 * x + 1 - y, 2 * (1 - x) + 1 - y
    native = c == x
    has_above, has_below = z < nz - 1, z > 0

    weights = (gate_ref, up_ref, down_ref)
    token_refs = (earlier_ref, cotangent_ref, later_ref)

    def remote(src, dst, send, recv, device):
        return pltpu.make_async_remote_copy(
            src_ref=src, dst_ref=dst, send_sem=send, recv_sem=recv, device_id=device, device_id_type=MESH
        )

    def each(k, body):
        if head == width:
            body(k, width)
            return

        @pl.when(k > 0)
        def _():
            body(k, width)

        @pl.when(k == 0)
        def _():
            body(k, head)

    def columns(k, size):
        return pl.ds(pl.multiple_of(jnp.maximum(k * width - (width - head), 0), 128), size)

    def block_rows(block, parity):
        return pl.ds(pl.multiple_of((block * 2 + parity) * depth, depth), depth)

    def slot(index):
        return pl.ds(pl.multiple_of(index * rows, rows), rows)

    barrier = pltpu.get_barrier_semaphore()
    for device in (pair, flip_x, flip_y, flip_both, partner):
        pl.semaphore_signal(barrier, inc=1, device_id=device, device_id_type=MESH)

    @pl.when(has_above)
    def _():
        pl.semaphore_signal(barrier, inc=1, device_id=above, device_id_type=MESH)

    @pl.when(has_below)
    def _():
        pl.semaphore_signal(barrier, inc=1, device_id=below, device_id_type=MESH)

    pl.semaphore_wait(barrier, 5 + jnp.where(has_above, 1, 0) + jnp.where(has_below, 1, 0))

    def swap(k, size, w):
        return remote(
            weights[w].at[:, columns(k, size)],
            full.at[w, block_rows(z, 1 - c), columns(k, size)],
            swap_send.at[w],
            swap_recv.at[k, w],
            partner,
        )

    def swap_arrival(k, size, w):
        return remote(
            weights[w].at[:, columns(k, size)],
            full.at[w, block_rows(z, c), columns(k, size)],
            swap_send.at[w],
            swap_recv.at[k, w],
            partner,
        )

    def own(w):
        return pltpu.make_async_copy(weights[w], full.at[w, block_rows(z, c)], own_sem.at[w])

    def start_swap(k):
        @pl.when(jnp.logical_not(native))
        def _():
            def body(k, size):
                for w in range(WEIGHTS):
                    swap(k, size, w).start()

            each(k, body)

    def token(a, way):
        device, at = ((flip_x, chip), (flip_y, chip), (flip_y, chip_x))[way]
        src = tokens.at[a, slot(chip_x)] if way == 2 else token_refs[a]
        return remote(src, tokens.at[a, slot(at)], token_send.at[a, way], token_recv.at[a, way], device)

    def token_arrival(a, way):
        at = (chip_x, chip_y, chip_both)[way]
        return remote(token_refs[a], tokens.at[a, slot(at)], token_send.at[a, way], token_recv.at[a, way], flip_x)

    def token_home(a):
        return pltpu.make_async_copy(token_refs[a], tokens.at[a, slot(chip)], token_own.at[a])

    @pl.when(native)
    def _():
        for w in range(WEIGHTS):
            own(w).start()

    for a in range(TOKENS_IN):
        token_home(a).start()
    start_swap(0)
    for a in range(2):
        token(a, 0).start()
        token(a, 1).start()
    lax.fori_loop(1, chunks, lambda k, _: (start_swap(k), 0)[1], 0)

    later_acc[...] = jnp.zeros_like(later_acc)
    input_acc[...] = jnp.zeros_like(input_acc)

    @pl.when(native)
    def _():
        for w in range(WEIGHTS):
            own(w).wait()

    def line(k, size, w, block, upward):
        where = full.at[w, block_rows(block, c), columns(k, size)]
        send = (up_send if upward else down_send).at[w, block]
        return remote(where, where, send, line_recv.at[k, w, block], above if upward else below)

    def across(k, size, w, block):
        where = full.at[w, block_rows(block, c), columns(k, size)]
        return remote(where, where, pair_send.at[w, block], pair_recv.at[k, w, block], pair)

    def across_arrival(k, size, w, block):
        where = full.at[w, block_rows(block, 1 - c), columns(k, size)]
        return remote(where, where, pair_send.at[w, block], pair_recv.at[k, w, block], pair)

    def send_own(k):
        def body(k, size):
            for w in range(WEIGHTS):
                @pl.when(jnp.logical_not(native))
                def _():
                    swap_arrival(k, size, w).wait_recv()

                @pl.when(has_above)
                def _():
                    line(k, size, w, z, True).start()

                @pl.when(has_below)
                def _():
                    line(k, size, w, z, False).start()

                across(k, size, w, z).start()

        each(k, body)

    def pass_on(k):
        def body(k, size):
            def step(d, _):
                for w in range(WEIGHTS):
                    @pl.when(z - d >= 0)
                    def _():
                        line(k, size, w, z - d, True).wait_recv()

                        @pl.when(has_above)
                        def _():
                            line(k, size, w, z - d, True).start()

                        across(k, size, w, z - d).start()

                    @pl.when(z + d <= nz - 1)
                    def _():
                        line(k, size, w, z + d, False).wait_recv()

                        @pl.when(has_below)
                        def _():
                            line(k, size, w, z + d, False).start()

                        across(k, size, w, z + d).start()

                return 0

            lax.fori_loop(1, nz, step, 0)

        each(k, body)

    def act(k, size, w):
        return remote(
            acts.at[w, 0, :, columns(k, size)],
            acts.at[w, 1, :, columns(k, size)],
            act_send.at[w],
            act_recv.at[k, w],
            pair,
        )

    def turn_ref(a, block):
        return other_tokens.at[a, :, pl.ds(block * depth, depth)]

    def other(a, block):
        return remote(
            tokens.at[a, :, block_rows(block, 1 - c)],
            turn_ref(a, block),
            other_send.at[a, block],
            other_recv.at[a, block],
            pair,
        )

    tiles = half // row_tile
    piece = 512 if model % 512 == 0 else model

    def tile_rows(r):
        return pl.ds(pl.multiple_of(r * row_tile, row_tile), row_tile)

    def by_columns_to(acc, where, pairs, cols):
        def step(n, _):
            out = pl.ds(pl.multiple_of(n * piece, piece), piece)
            value = acc[where, out]
            for left, w in pairs:
                value = value + lax.dot_general(
                    left, full[w, out, cols], (((1,), (1,)), ((), ())), preferred_element_type=jnp.float32
                )
            acc[where, out] = value
            return 0

        lax.fori_loop(0, model // piece, step, 0)

    def earlier(k):
        def body(k, size):
            cols = columns(k, size)

            def wait_block(block, _):
                for w in range(WEIGHTS):
                    across_arrival(k, size, w, block).wait_recv()
                return 0

            lax.fori_loop(0, nz, wait_block, 0)

            def tile(r, _):
                where = tile_rows(r)
                gate = dot(tokens[0, where, :], full[0, :, cols])
                lift = dot(tokens[0, where, :], full[1, :, cols])
                back = dot(tokens[1, where, :], full[2, :, cols])
                active, slope = silu_parts(gate)
                acts[2, 0, where, cols] = (active * lift).astype(jnp.bfloat16)
                gate_back = (back * lift * slope).astype(jnp.bfloat16)
                up_back = (back * active).astype(jnp.bfloat16)
                acts[0, 0, where, cols] = gate_back
                acts[1, 0, where, cols] = up_back
                return 0

            lax.fori_loop(0, tiles, tile, 0)
            for w in range(WEIGHTS):
                act(k, size, w).start()

            def finish(r, _):
                where = tile_rows(r)
                by_columns_to(input_acc, where, ((acts[0, 0, where, cols], 0), (acts[1, 0, where, cols], 1)), cols)
                return 0

            lax.fori_loop(0, tiles, finish, 0)

        each(k, body)

    def later(k):
        def body(k, size):
            cols = columns(k, size)

            def tile(r, _):
                where = tile_rows(r)
                gate = dot(tokens[2, where, :], full[0, :, cols])
                lift = dot(tokens[2, where, :], full[1, :, cols])
                hidden = (jax.nn.silu(gate) * lift).astype(jnp.bfloat16)
                by_columns_to(later_acc, where, ((hidden, 2),), cols)
                return 0

            lax.fori_loop(0, tiles, tile, 0)

        each(k, body)

    def part(o, way):
        device, at = ((flip_y, chip_y), (flip_y, chip_both), (flip_x, chip_x))[way]
        return remote(
            tokens.at[(2, 0)[o], slot(at)], parts_in.at[o, way], part_send.at[o, way], part_recv.at[o, way], device
        )

    def combine_parts(o):
        part(o, 1).wait_recv()
        mine = slot(chip_x)
        total = tokens[(2, 0)[o], mine, :].astype(jnp.float32) + parts_in[o, 1].astype(jnp.float32)
        tokens[(2, 0)[o], mine, :] = total.astype(jnp.bfloat16)
        part(o, 2).start()

    def send_parts(o):
        acc = (later_acc, input_acc)[o]

        def step(r, _):
            where = tile_rows(r)
            tokens[(2, 0)[o], where, :] = acc[where, :].astype(jnp.bfloat16)
            return 0

        lax.fori_loop(0, tiles, step, 0)
        for way in (1, 0):
            part(o, way).start()

    def running(k, size, w, index, device):
        where = sums.at[w, index, :, columns(k, size)]
        return remote(where, where, sum_send.at[w, index], sum_recv.at[k, w, index], device)

    home = jnp.where(has_above, nz - 1 + z, z - 1)

    def give(k, size, w):
        cols = columns(k, size)
        return remote(sums.at[w, home, :, cols], final.at[w, :, cols], final_send.at[w], final_recv.at[w], partner)

    def product(k, size, w, target):
        source = 1 if w == 2 else 0
        cols = columns(k, size)
        value = dot(turned[source, target, 0], acts[w, 0, :, cols])
        return value + dot(turned[source, target, 1], acts[w, 1, :, cols])

    def add_arrived(k, size, w, index, device, here):
        running(k, size, w, index, device).wait_recv()
        dots[:, here] += sums[w, index, :, columns(k, size)].astype(jnp.float32)

    def reduce(k, first):
        def body(k, size):
            here = pl.ds(0, size)

            @pl.when(first)
            def _():
                for w in range(WEIGHTS):
                    act(k, size, w).wait_recv()

            def phase():
                upward = first == (2 * z < nz - 1)
                count = jnp.where(upward, nz - 1 - z, z)
                has_previous = jnp.where(upward, z, nz - 1 - z) > 0
                device = (z + jnp.where(upward, 1, -1), x, y, c)

                def send(m, _):
                    target = jnp.where(upward, nz - 1 - m, m)
                    index = jnp.where(upward, target - 1, nz - 1 + target)
                    for w in (2, 0, 1):
                        dots[:, here] = product(k, size, w, target)

                        @pl.when(has_previous)
                        def _():
                            add_arrived(k, size, w, index, device, here)

                        sums[w, index, :, columns(k, size)] = dots[:, here].astype(jnp.bfloat16)
                        running(k, size, w, index, device).start()
                    return 0

                lax.fori_loop(0, count, send, 0)

            phase()

        each(k, body)

    def finish_sum(k):
        def body(k, size):
            cols = columns(k, size)
            here = pl.ds(0, size)
            for w in (2, 0, 1):
                dots[:, here] = product(k, size, w, z)

                @pl.when(has_below)
                def _():
                    add_arrived(k, size, w, z - 1, below, here)

                @pl.when(has_above)
                def _():
                    add_arrived(k, size, w, nz - 1 + z, above, here)

                @pl.when(native)
                def _():
                    final[w, :, cols] = dots[:, here].astype(jnp.bfloat16)

                @pl.when(jnp.logical_not(native))
                def _():
                    sums[w, home, :, cols] = dots[:, here].astype(jnp.bfloat16)
                    give(k, size, w).start()

        each(k, body)

    def forward_token(a):
        token_arrival(a, 0).wait_recv()
        token(a, 2).start()

    middle = jnp.logical_and(has_above, has_below)
    border = jnp.logical_not(middle)
    foreign = jnp.logical_not(native)
    send_own(0)

    @pl.when(native)
    def _():
        send_own(1)

    forward_token(0)

    @pl.when(middle)
    def _():
        pass_on(0)

    forward_token(1)

    @pl.when(foreign)
    def _():
        send_own(1)

    @pl.when(border)
    def _():
        @pl.when(native)
        def _():
            lax.fori_loop(2, chunks, lambda k, _: (send_own(k), 0)[1], 0)

        pass_on(0)

        @pl.when(foreign)
        def _():
            lax.fori_loop(2, min(2 + 2, chunks), lambda k, _: (send_own(k), 0)[1], 0)

    token(2, 0).start()
    token(2, 1).start()

    @pl.when(middle)
    def _():
        lax.fori_loop(2, min(1 + lead, chunks), lambda k, _: (send_own(k), 0)[1], 0)

        def step(k, _):
            @pl.when(k + lead < chunks)
            def _():
                send_own(k + lead)

            pass_on(k)
            return 0

        lax.fori_loop(1, ahead, step, 0)

    for a in range(2):
        token_home(a).wait()
        token_arrival(a, 1).wait_recv()
        token_arrival(a, 2).wait_recv()
        for block in range(nz):
            other(a, block).start()
    for a in range(2):
        for block in range(nz):
            turned[a, block, 0] = tokens[a, :, block_rows(block, c)].T
    for a in range(2):
        for block in range(nz):
            other(a, block).wait()
            turned[a, block, 1] = other_tokens[a, :, block * depth : (block + 1) * depth].T
    for a in range(2):
        for way in range(3):
            token(a, way).wait_send()

    def span(i):
        return jnp.clip(jnp.minimum(pace * (i - hold), i - 2), 0, chunks)

    def iteration(i, _):
        @pl.when(i < chunks)
        def _():
            earlier(i)

        @pl.when(jnp.logical_and(i == 0, jnp.logical_and(foreign, border)))
        def _():
            lax.fori_loop(min(2 + 2, chunks), chunks, lambda k, _: (send_own(k), 0)[1], 0)

        @pl.when(i == chunks - 1)
        def _():
            send_parts(1)

        @pl.when(i == chunks)
        def _():
            combine_parts(1)

        @pl.when(jnp.logical_and(middle, i + ahead < chunks))
        def _():
            @pl.when(i + ahead + lead < chunks)
            def _():
                send_own(i + ahead + lead)

            pass_on(i + ahead)

        @pl.when(i == 1)
        def _():
            token_home(2).wait()
            token_arrival(2, 1).wait_recv()
            token_arrival(2, 2).wait_recv()
            for way in range(3):
                token(2, way).wait_send()

        near = jnp.where(jnp.logical_and(i >= lag, i - lag < chunks), 1, 0)
        far = jnp.where(middle, span(i), span(i + 1))

        def send_sums(n, _):
            first = n < near
            reduce(jnp.where(first, i - lag, far + n - near), first)
            return 0

        lax.fori_loop(0, near + span(i + 1) - far, send_sums, 0)

        lax.fori_loop(
            jnp.maximum(i - 1, 0),
            jnp.where(i == chunks - 1, chunks, jnp.where(i < chunks, i, 0)),
            lambda k, _: (later(k), 0)[1],
            0,
        )

        @pl.when(i == chunks - 1)
        def _():
            send_parts(0)

        @pl.when(i == 0)
        def _():
            forward_token(2)

        @pl.when(jnp.logical_and(border, i + 1 < chunks))
        def _():
            pass_on(i + 1)

        @pl.when(i == chunks)
        def _():
            combine_parts(0)

        done = jnp.where(middle, jnp.clip(i - late, 0, chunks), jnp.where(i < chunks, 0, span(i - 1)))
        ready = jnp.where(middle, jnp.clip(i + 1 - late, 0, chunks), jnp.where(i + 1 < chunks, 0, span(i)))
        lax.fori_loop(done, ready, lambda k, _: (finish_sum(k), 0)[1], 0)
        return 0

    lag = jnp.where(middle, 1, 0)
    late = 3
    lax.fori_loop(0, chunks + late, iteration, 0)

    for o, out_ref in ((1, input_grad_ref), (0, later_out_ref)):
        part(o, 1).wait_send()
        part(o, 0).wait()
        part(o, 2).wait()
        mine = slot(chip)
        total = tokens[(2, 0)[o], mine, :].astype(jnp.float32)
        for way in (0, 2):
            total = total + parts_in[o, way].astype(jnp.float32)
        parts_in[o, 0] = total.astype(jnp.bfloat16)
        pltpu.make_async_copy(parts_in.at[o, 0], out_ref, out_sem.at[o]).start()

    @pl.when(foreign)
    def _():
        for w in range(WEIGHTS):
            whole = remote(sums.at[w, home], final.at[w], final_send.at[w], final_recv.at[w], partner)
            whole.wait_send()
            whole.wait_recv()

    for w, out_ref in enumerate((gate_sum_ref, up_sum_ref, down_sum_ref)):
        pltpu.make_async_copy(final.at[w], out_ref, out_sem.at[2 + w]).start()

    for w in range(WEIGHTS):
        remote(acts.at[w, 0], acts.at[w, 1], act_send.at[w], act_recv.at[0, w], pair).wait_send()

        @pl.when(foreign)
        def _():
            remote(
                weights[w], full.at[w, block_rows(z, 1 - c)], swap_send.at[w], swap_recv.at[0, w], partner
            ).wait_send()

        def block_sends(block, _):
            where = full.at[w, block_rows(block, c)]
            remote(where, where, pair_send.at[w, block], pair_recv.at[0, w, block], pair).wait_send()

            @pl.when(jnp.logical_and(has_above, block <= z))
            def _():
                remote(where, where, up_send.at[w, block], line_recv.at[0, w, block], above).wait_send()

            @pl.when(jnp.logical_and(has_below, block >= z))
            def _():
                remote(where, where, down_send.at[w, block], line_recv.at[0, w, block], below).wait_send()

            @pl.when(block != z)
            def _():
                index = jnp.where(block > z, block - 1, nz - 1 + block)
                where = sums.at[w, index]
                device = (z + jnp.where(block > z, 1, -1), x, y, c)
                remote(where, where, sum_send.at[w, index], sum_recv.at[0, w, index], device).wait_send()

            return 0

        lax.fori_loop(0, nz, block_sends, 0)

    for o, out_ref in ((1, input_grad_ref), (0, later_out_ref)):
        pltpu.make_async_copy(parts_in.at[o, 0], out_ref, out_sem.at[o]).wait()
    for w, out_ref in enumerate((gate_sum_ref, up_sum_ref, down_sum_ref)):
        pltpu.make_async_copy(final.at[w], out_ref, out_sem.at[2 + w]).wait()


def fused(nz, later_rows, earlier_rows, cotangent, gate_weight, up_weight, down_weight):
    rows, model = later_rows.shape
    depth, ff = gate_weight.shape
    half = 4 * rows
    width = 256 if ff > 256 else ff
    chunks = -(-ff // width)
    row_tile = half // 2 if (half // 2) % 16 == 0 else half
    dma = pltpu.SemaphoreType.DMA
    bf16, f32 = jnp.bfloat16, jnp.float32
    scratch = [
        pltpu.VMEM((WEIGHTS, model, ff), bf16),
        pltpu.VMEM((TOKENS_IN, half, model), bf16),
        pltpu.VMEM((2, half, nz * depth), bf16),
        pltpu.VMEM((2, nz, 2, depth, half), bf16),
        pltpu.VMEM((WEIGHTS, 2, half, ff), bf16),
        pltpu.VMEM((WEIGHTS, 2 * (nz - 1), depth, ff), bf16),
        pltpu.VMEM((half, model), f32),
        pltpu.VMEM((half, model), f32),
        pltpu.VMEM((2, 3, rows, model), bf16),
        pltpu.VMEM((WEIGHTS, depth, ff), bf16),
        pltpu.VMEM((depth, width), f32),
        dma((WEIGHTS,)),
        dma((WEIGHTS,)),
        dma((chunks, WEIGHTS)),
        dma((chunks, WEIGHTS, nz)),
        dma((chunks, WEIGHTS, nz)),
        dma((WEIGHTS, nz)),
        dma((WEIGHTS, nz)),
        dma((WEIGHTS, nz)),
        dma((TOKENS_IN,)),
        dma((TOKENS_IN, 3)),
        dma((TOKENS_IN, 3)),
        dma((2, nz)),
        dma((2, nz)),
        dma((WEIGHTS,)),
        dma((chunks, WEIGHTS)),
        dma((WEIGHTS, 2 * (nz - 1))),
        dma((chunks, WEIGHTS, 2 * (nz - 1))),
        dma((WEIGHTS,)),
        dma((WEIGHTS,)),
        dma((2, 3)),
        dma((2, 3)),
        dma((5,)),
    ]
    return pl.pallas_call(
        functools.partial(fused_kernel, nz, width, min(4, chunks - 1), row_tile),
        out_shape=[jax.ShapeDtypeStruct((rows, model), bf16)] * 2
        + [jax.ShapeDtypeStruct((depth, ff), bf16)] * 3,
        in_specs=[pl.BlockSpec(memory_space=pl.ANY)] * 6,
        out_specs=[pl.BlockSpec(memory_space=pl.ANY)] * 5,
        scratch_shapes=scratch,
        compiler_params=pltpu.CompilerParams(
            collective_id=0, has_side_effects=True, vmem_limit_bytes=67_000_000
        ),
        cost_estimate=pl.CostEstimate(flops=22 * half * model * ff, bytes_accessed=0, transcendentals=0),
    )(later_rows, earlier_rows, cotangent, gate_weight, up_weight, down_weight)


def general(mesh):
    nf, nt = mesh.shape["fs"], mesh.shape["tp"]
    nx = max(d for d in range(1, nf + 1) if nf % d == 0 and d * d <= nf)
    nz = nf // nx
    split = Mesh(mesh.devices.reshape(nz, nx, nt), ("z", "x", "tp"))
    plane = ("x", "tp")

    def local(
        later_rows,
        earlier_rows,
        cotangent,
        gate_weight,
        up_weight,
        down_weight,
        gate_grad_sum,
        up_grad_sum,
        down_grad_sum,
    ):
        gate_full, gate_last = gather_line(spread_columns(gate_weight, nx), nz)
        up_full, up_last = gather_line(spread_columns(up_weight, nx), nz)
        rows_all = lax.all_gather(earlier_rows, plane, axis=0, tiled=True)
        back_all = lax.all_gather(cotangent, plane, axis=0, tiled=True)
        piece = lax.all_gather(after(later_rows, *gate_last), plane, axis=0, tiled=True)

        gate_e = dot(rows_all, gate_full)
        up_e = dot(rows_all, up_full)
        activation, act_slope = silu_parts(gate_e)
        hidden_e = (activation * up_e).astype(jnp.bfloat16)
        down_parts = by_rows(back_all, hidden_e)
        down_grad, down_first = scatter_line(down_parts, nz)
        later_hidden = (jax.nn.silu(dot(piece, gate_full)) * dot(piece, up_full)).astype(jnp.bfloat16)
        down_block = after(spread_columns(down_weight, nx), *gate_last, *up_last)
        down_full, _ = gather_line(down_block, nz, lambda: ((gate_e, up_e), (down_parts, later_hidden) + down_first))
        later_parts = by_columns(later_hidden, down_full).astype(jnp.bfloat16)
        later_out = lax.psum_scatter(later_parts, plane, scatter_dimension=0, tiled=True)
        back_hidden = dot(back_all, down_full)
        gate_back = (back_hidden * up_e * act_slope).astype(jnp.bfloat16)
        up_back = (back_hidden * activation).astype(jnp.bfloat16)
        gate_parts = by_rows(rows_all, gate_back)
        up_parts = by_rows(rows_all, up_back)
        gate_grad, gate_first = scatter_line(gate_parts, nz)
        up_grad, _ = scatter_line(up_parts, nz)
        gate_back = after(gate_back, *gate_first)
        up_back = after(up_back, *gate_first)
        input_grad = lax.psum_scatter(
            after(
                (by_columns(gate_back, gate_full) + by_columns(up_back, up_full)).astype(jnp.bfloat16),
                later_out,
            ),
            plane,
            scatter_dimension=0,
            tiled=True,
        )
        return (
            later_out,
            input_grad,
            gate_grad_sum + join_columns(gate_grad, nx),
            up_grad_sum + join_columns(up_grad, nx),
            down_grad_sum + join_columns(down_grad, nx),
        )

    rows, weights = P(("z", "x", "tp"), None), P(("z", "x"), "tp")
    return jax.shard_map(
        local,
        mesh=split,
        in_specs=(rows,) * 3 + (weights,) * 6,
        out_specs=(rows,) * 2 + (weights,) * 3,
        check_vma=False,
    )


def solution(mesh):
    nf, nt = mesh.shape["fs"], mesh.shape["tp"]
    nx = max(d for d in range(1, nf + 1) if nf % d == 0 and d * d <= nf)
    nz = nf // nx
    if nx != 2 or nt != 4 or nz < 2:
        return general(mesh)
    split = Mesh(mesh.devices.reshape(nz, 2, 2, 2), ("z", "x", "y", "c"))

    def local(later_rows, earlier_rows, cotangent, gate, up, down, *grad_sums):
        later_out, input_grad, *totals = fused(nz, later_rows, earlier_rows, cotangent, gate, up, down)
        return (later_out, input_grad, *(s + t.astype(jnp.float32) for s, t in zip(grad_sums, totals)))

    rows, weights = P(("z", "x", "y", "c"), None), P(("z", "x"), ("y", "c"))
    return jax.shard_map(
        local,
        mesh=split,
        in_specs=(rows,) * 3 + (weights,) * 6,
        out_specs=(rows,) * 2 + (weights,) * 3,
        check_vma=False,
    )
```
